32 devices in a mesh: ep: 8 (over z, core), tp: 4 (over y, x).
Axes of the slice: x: 2, y: 2, z: 4, core: 2. Of those that a mesh axis runs over, the one named last changes fastest.
Arguments:
- tokens: bfloat16 [64, 2048], P('ep'), may hold values from -6 to 6
- attn_gain: float32 [2048], replicated, may hold values from 0.1 to 1.9
- query_weight: bfloat16 [2048, 4096], P('ep', 'tp'), may hold values from -0.125 to 0.125
- key_weight: bfloat16 [2048, 4096], P('ep', 'tp'), may hold values from -0.125 to 0.125
- value_weight: bfloat16 [2048, 4096], P('ep', 'tp'), may hold values from -0.125 to 0.125
- query_gain: float32 [128], replicated, may hold values from 0.1 to 1.9
- stick_bias: float32 [32], P('tp'), may hold values from -7 to -2.5
- key_cache: bfloat16 [64, 32, 512, 128], P('ep', 'tp'), may hold values from -6 to 6
- value_cache: bfloat16 [64, 32, 512, 128], P('ep', 'tp'), may hold values from -6 to 6
- lengths: int32 [64], P('ep'), may hold values from 64 to 512, as said below
- out_weight: bfloat16 [4096, 2048], P('tp'), may hold values from -0.375 to 0.375
- mix_gain: float32 [2048], replicated, may hold values from 0.1 to 1.9
- route_ids: int32 [64, 2], P('ep'), may hold values from 0 to 7, all different within a row; in each aligned block of 8 rows (0 to 7, 8 to 15, ...) at most 4 rows name the same one
- route_weights: float32 [64, 2], P('ep'), may hold values from 0.2 to 1
- expert_gate: bfloat16 [8, 2048, 2560], P('ep', None, 'tp'), may hold values from -0.125 to 0.125
- expert_up: bfloat16 [8, 2048, 2560], P('ep', None, 'tp'), may hold values from -0.125 to 0.125
- expert_down: bfloat16 [8, 2560, 2048], P('ep', 'tp'), may hold values from -0.15625 to 0.15625
- side_gate: bfloat16 [2048, 1024], P(None, 'tp'), may hold values from -0.125 to 0.125
- side_up: bfloat16 [2048, 1024], P(None, 'tp'), may hold values from -0.125 to 0.125
- side_down: bfloat16 [1024, 2048], P('tp'), may hold values from -0.25 to 0.25
- branch_gate: float32 [2048], replicated, may hold values from -0.125 to 0.125
Outputs:
- mixed: bfloat16 [64, 2048], P('ep', 'tp')
- new_keys: bfloat16 [64, 4096], P('ep', 'tp')
- new_values: bfloat16 [64, 4096], P('ep', 'tp')
The draws below stay inside these ranges and needn't reach their ends.
Inputs may be any that keep to these rules, and one draw needn't show every extreme that they name: `lengths`: at least an eighth of 512; the first sequence has 512. `route_ids`: each token names 2 different experts. In the rows of one device no expert is named by more than 4 rows, a bound that some block reaches of some device.
All inputs are finite; a program needn't handle non-finite values.
Results may differ from the reference program's by a relative error of at most 0.018.
Values may be sent and summed in bfloat16 or wider, within the bound.
No kernel may reach another device: no remote copies, remote signals or barrier semaphores. Data moves between devices by JAX's collectives and lax.ppermute only.
A program may use at most 64 MiB of HBM per device.

```python
import math
import jax
import jax.numpy as jnp
import numpy as np
from jax import lax

D = 2048
H = 32
DH = 128
FF_E = 2560
SH = 1024
TOP = 2
SEQS = 8
L = 512
BATCH = 64
E = 8
CAP = 4
N_EP = 8


def draw_lengths(key, part):
    drawn = jax.random.randint(key, (BATCH,), L // 8, L + 1, dtype=jnp.int32)
    return drawn.at[0].set(L)


def raised(result, key, source, target, shards_of, factor):
    owner, partner = [(jnp.arange(result.shape[axis_at]) // (result.shape[axis_at] // shards_of)).reshape([-1 if axis == axis_at else 1 for axis in range(result.ndim)]) for axis_at in (source, target)]
    chosen = jax.random.permutation(key, shards_of)[partner]
    strong = (owner == chosen) | (owner == (partner + shards_of // 2) % shards_of)
    return jnp.where(strong, factor * result, result)


def level_of(key, dims, pieces, low, high):
    gain = 1.0
    for axis_at, parts in pieces:
        steps = jax.random.uniform(jax.random.fold_in(jax.random.fold_in(key, 6), axis_at), (parts,), jnp.float32, low / len(pieces), high / len(pieces))
        gain = gain * jnp.repeat(jnp.exp(steps), dims[axis_at] // parts).reshape((-1,) + (1,) * (len(dims) - 1 - axis_at))
    return gain


def routed_block(own_key, own, number, rows, amount, top, bound, lean):
    ranking = jax.random.permutation(own_key, amount)
    crowded, ordinary = portions_of(amount, rows * top, bound, lean, True), portions_of(amount, rows * top, bound, lean, False)
    places = jnp.arange(amount)

    def named(sizes, rotation):
        used = int((sizes > 0).sum())
        fixed = max(1, used // 4)
        moved = fixed + (places - fixed + rotation * (used - fixed)) % max(1, amount - fixed)
        return jnp.zeros((amount,), jnp.int32).at[ranking[jnp.where(places < fixed, places, moved)]].set(jnp.asarray(sizes, jnp.int32))

    sizes = jnp.where(number % 4 == 0, named(crowded, number // 4), named(ordinary, number - number // 4 - 1))
    mixed = jax.random.permutation(jax.random.fold_in(own, 3), amount)
    source_of, receiver = mixed[0:amount // 2 * 2:2], mixed[1:amount // 2 * 2:2]
    margin = jnp.minimum(sizes[source_of] - 1, bound - sizes[receiver]) // 2
    margin = jnp.where((source_of == ranking[0]) | (receiver == ranking[0]) | (sizes[receiver] == 0), 0, jnp.maximum(margin, 0))
    moved = jax.random.randint(jax.random.fold_in(own, 4), (amount // 2,), 0, 1 << 20) % (margin + 1)
    sizes = sizes.at[source_of].add(-moved).at[receiver].add(moved)
    items = jnp.searchsorted(jnp.cumsum(sizes), jnp.arange(rows * top), side="right").astype(jnp.int32)
    grid = items.reshape(top, rows).T
    grid = grid[jax.random.permutation(jax.random.fold_in(own, 1), rows)]
    rotation = jax.random.randint(jax.random.fold_in(own, 2), (rows, 1), 0, top)
    return jnp.take_along_axis(grid, (jnp.arange(top)[None, :] + rotation) % top, axis=1)


def portions_of(number_of, total, limit, slope, full):
    weights = [(1 << 20) // math.isqrt(standing ** slope) + 1 for standing in range(1, number_of + 1)]
    largest = limit if full else min(limit, max(-(-total // number_of), total * weights[0] // sum(weights)))
    least = 1 if total - largest >= number_of - 1 else 0
    counts, rest = [largest] + [least] * (number_of - 1), total - largest - least * (number_of - 1)
    while rest > 0:
        candidates = [i for i in range(1, number_of) if counts[i] < largest] or [i for i in range(1, number_of) if counts[i] < limit]
        pool, remaining = sum([weights[i] for i in candidates]), rest
        for i in candidates:
            addition = min(limit - counts[i], max(1, remaining * weights[i] // pool), rest)
            counts[i] = counts[i] + addition
            rest = rest - addition
    return np.array(counts)


def gaussian(key, extent, deviation, reach, split=(), kind=jnp.bfloat16):
    level = level_of(key, extent, split, -0.22, 0.18) if split else 1.0
    entries = jax.random.normal(key, extent, jnp.float32) * deviation * level
    return jnp.minimum(jnp.maximum(entries, -reach), reach).astype(kind)


def gaussian_with(own_key, shape, deviation, limit, split, heavy, held_as=jnp.bfloat16):
    entries = deviation * jax.random.normal(own_key, shape, jnp.float32)
    if split:
        entries = entries * level_of(own_key, shape, split, -0.22, 0.18)
    return jnp.clip(raised(entries, jax.random.fold_in(own_key, 3), *heavy), -limit, limit).astype(held_as)


def setup_inputs(seed: int = 0) -> dict:
    keys = jax.random.split(jax.random.key(seed), 22)
    tokens = gaussian(keys[0], (BATCH, D), 1.0, 6.0, ((0, 8),))
    attn_gain = jnp.clip(1.0 + 0.18 * jax.random.normal(keys[1], (D,), jnp.float32), 0.1, 1.9)
    query_weight = gaussian(keys[2], (D, H * DH), D ** -0.5, 0.125, ((0, 8), (1, 4)))
    key_weight = gaussian(keys[3], (D, H * DH), D ** -0.5, 0.125, ((0, 8), (1, 4)))
    value_weight = gaussian(keys[4], (D, H * DH), D ** -0.5, 0.125, ((0, 8), (1, 4)))
    query_gain = jnp.clip(1.0 + 0.18 * jax.random.normal(keys[5], (DH,), jnp.float32), 0.1, 1.9)
    stick_bias = jnp.clip(-7.0 + 4.5 * jax.random.uniform(keys[6], (H,), jnp.float32) ** level_of(keys[6], (H,), ((0, 4),), -0.2, 0.2), -7.0, -2.5)
    key_cache = gaussian(keys[7], (BATCH, H, L, DH), 1.0, 6.0, ((0, 8), (1, 4)))
    value_cache = gaussian(keys[8], (BATCH, H, L, DH), 1.0, 6.0, ((0, 8), (1, 4)))
    lengths = draw_lengths(jax.random.fold_in(keys[21], 71), 0)
    out_weight = gaussian(keys[10], (H * DH, D), (H * DH // 16) ** -0.5, 0.375, ((0, 4),))
    mix_gain = jnp.clip(1.0 + 0.18 * jax.random.normal(keys[11], (D,), jnp.float32), 0.1, 1.9)
    route_ids_keys = jax.random.split(jax.random.fold_in(keys[12], 1), BATCH // SEQS)
    route_ids_turns = jax.random.permutation(jax.random.fold_in(keys[12], 3), BATCH // SEQS)
    route_ids = jax.vmap(lambda own, number: routed_block(jax.random.fold_in(keys[12], 2), own, number, SEQS, E, TOP, CAP, 2))(route_ids_keys, route_ids_turns).reshape((BATCH, TOP))
    route_weights = jnp.clip(0.2 + 0.8 * jax.random.uniform(keys[13], (BATCH, TOP), jnp.float32) ** level_of(keys[13], (BATCH, TOP), ((0, 8),), -0.2, 0.2), 0.2, 1.0)
    expert_gate = gaussian(keys[14], (E, D, FF_E), D ** -0.5, 0.125, ((0, 8), (2, 4)))
    expert_up = gaussian(keys[15], (E, D, FF_E), D ** -0.5, 0.125, ((0, 8), (2, 4)))
    expert_down = gaussian_with(keys[16], (E, FF_E, D), FF_E ** -0.5, 0.15625, ((0, 8), (1, 4)), (1, 2, 4, 2.0))
    side_gate = gaussian(keys[17], (D, SH), D ** -0.5, 0.125, ((1, 4),))
    side_up = gaussian(keys[18], (D, SH), D ** -0.5, 0.125, ((1, 4),))
    side_down = gaussian_with(keys[19], (SH, D), SH ** -0.5, 0.25, ((0, 4),), (0, 1, 4, 2.0))
    branch_gate = gaussian(keys[20], (D,), D ** -0.5, 0.125, (), jnp.float32)
    return dict(tokens=tokens, attn_gain=attn_gain, query_weight=query_weight, key_weight=key_weight, value_weight=value_weight, query_gain=query_gain, stick_bias=stick_bias, key_cache=key_cache, value_cache=value_cache, lengths=lengths, out_weight=out_weight, mix_gain=mix_gain, route_ids=route_ids, route_weights=route_weights, expert_gate=expert_gate, expert_up=expert_up, expert_down=expert_down, side_gate=side_gate, side_up=side_up, side_down=side_down, branch_gate=branch_gate)


epsilon = 1e-06

def rms_scale(values, scale_gain):
    mean_square = lax.optimization_barrier(jnp.mean(values * values, axis=-1, keepdims=True))
    return values * lax.rsqrt(mean_square + epsilon) * scale_gain

def expert_apply(bundle):
    slot_rows, gate_w, up_w, down_w = bundle
    gate_pre = jnp.dot(slot_rows, gate_w, preferred_element_type=jnp.float32)
    up_pre = jnp.dot(slot_rows, up_w, preferred_element_type=jnp.float32)
    hidden = (jax.nn.silu(gate_pre) * up_pre).astype(jnp.bfloat16)
    return jnp.dot(hidden, down_w, preferred_element_type=jnp.float32).astype(jnp.bfloat16)

def reference(tokens, attn_gain, query_weight, key_weight, value_weight, query_gain, stick_bias, key_cache, value_cache, lengths, out_weight, mix_gain, route_ids, route_weights, expert_gate, expert_up, expert_down, side_gate, side_up, side_down, branch_gate):
    stream = tokens.astype(jnp.float32)
    normed = rms_scale(stream, attn_gain).astype(jnp.bfloat16)
    query_rows = jnp.dot(normed, query_weight, preferred_element_type=jnp.float32).astype(jnp.bfloat16)
    fresh_keys = jnp.dot(normed, key_weight, preferred_element_type=jnp.float32).astype(jnp.bfloat16)
    new_values = jnp.dot(normed, value_weight, preferred_element_type=jnp.float32).astype(jnp.bfloat16)
    batch_count = tokens.shape[0]
    new_keys = rms_scale(fresh_keys.astype(jnp.float32).reshape(batch_count, H, DH), 1.0)
    new_keys = new_keys.astype(jnp.bfloat16).reshape(batch_count, H * DH)
    query_heads = rms_scale(query_rows.astype(jnp.float32).reshape(batch_count, H, DH), query_gain)
    query_heads = query_heads.astype(jnp.bfloat16)

    def attend_one(bundle):
        query_row, key_rows, value_rows, length = bundle
        scores = jnp.einsum('hd,hld->hl', query_row.astype(jnp.float32), key_rows.astype(jnp.float32))
        scores = scores * DH ** (-0.5) + stick_bias[:, None]
        positions = jnp.arange(L, dtype=jnp.int32)
        visible = positions[None, :] < length
        log_rest = jnp.where(visible, jax.nn.log_sigmoid(-scores), 0.0)
        log_between = lax.cumsum(log_rest, axis=1, reverse=True) - log_rest
        stick = jnp.where(visible, jnp.exp(jax.nn.log_sigmoid(scores) + log_between), 0.0).astype(jnp.bfloat16)
        attended = jnp.einsum('hl,hld->hd', stick.astype(jnp.float32), value_rows.astype(jnp.float32))
        return attended.astype(jnp.bfloat16).reshape(H * DH)
    attended = lax.map(attend_one, (query_heads, key_cache, value_cache, lengths))
    attn_proj = jnp.dot(attended, out_weight, preferred_element_type=jnp.float32)
    middle = (stream + attn_proj).astype(jnp.bfloat16)
    normed_mix = rms_scale(middle.astype(jnp.float32), mix_gain).astype(jnp.bfloat16)
    flat_ids = route_ids.reshape(N_EP, SEQS * TOP)
    onehot = (flat_ids[:, :, None] == jnp.arange(E, dtype=jnp.int32)[None, None, :]).astype(jnp.int32)
    before = jnp.cumsum(onehot, axis=1) - onehot
    slot_index = lax.optimization_barrier(jnp.sum(before * onehot, axis=2))
    sources = jnp.arange(N_EP, dtype=jnp.int32)[:, None]
    target = ((flat_ids * N_EP + sources) * CAP + slot_index).reshape(-1).astype(jnp.int32)
    slot_table = jnp.zeros((E * N_EP * CAP,), jnp.int32).at[target].set(jnp.arange(BATCH * TOP, dtype=jnp.int32))
    slot_rows = normed_mix[slot_table // TOP].reshape(E, N_EP * CAP, D)
    expert_outs = lax.map(expert_apply, (slot_rows, expert_gate, expert_up, expert_down))
    route_out = expert_outs.reshape(E * N_EP * CAP, D)[target].astype(jnp.float32).reshape(BATCH, TOP, D)
    routed = lax.optimization_barrier(jnp.sum(route_weights[:, :, None] * route_out, axis=1))
    side_gate_pre = jnp.dot(normed_mix, side_gate, preferred_element_type=jnp.float32)
    side_up_pre = jnp.dot(normed_mix, side_up, preferred_element_type=jnp.float32)
    side_hidden = (jax.nn.silu(side_gate_pre) * side_up_pre).astype(jnp.bfloat16)
    side_out = jnp.dot(side_hidden, side_down, preferred_element_type=jnp.float32)
    switch = jax.nn.sigmoid(lax.optimization_barrier(jnp.sum(normed_mix.astype(jnp.float32) * branch_gate, axis=1, keepdims=True)))
    mixed = (middle.astype(jnp.float32) + routed + switch * side_out).astype(jnp.bfloat16)
    return (mixed, new_keys, new_values)
```

```python
import jax
import jax.numpy as jnp
from jax import lax
from jax.sharding import PartitionSpec as P

DH = 128


epsilon = 1e-06


def rms_scale(values, scale_gain):
    mean_square = jnp.mean(values * values, axis=-1, keepdims=True)
    return values * lax.rsqrt(mean_square + epsilon) * scale_gain


def summed_blocks(partial, axis_name):
    count = lax.axis_size(axis_name)
    rows = partial.shape[0] // count
    blocks = lax.all_to_all(
        partial.astype(jnp.bfloat16), axis_name, split_axis=0, concat_axis=0, tiled=True
    )
    return jnp.sum(blocks.reshape(count, rows, -1).astype(jnp.float32), axis=0)


def body(
    tokens,
    attn_gain,
    query_weight,
    key_weight,
    value_weight,
    query_gain,
    stick_bias,
    key_cache,
    value_cache,
    lengths,
    out_weight,
    mix_gain,
    route_ids,
    route_weights,
    expert_gate,
    expert_up,
    expert_down,
    side_gate,
    side_up,
    side_down,
    branch_gate,
):
    seq_count, model_width = tokens.shape
    head_cols = query_weight.shape[1]
    heads_local = key_cache.shape[1]
    cache_slots = key_cache.shape[2]
    experts = lax.axis_size("ep")
    tp_size = lax.axis_size("tp")
    stream = tokens.astype(jnp.float32)
    normed = rms_scale(stream, attn_gain).astype(jnp.bfloat16)
    columns = lax.all_to_all(normed, "ep", split_axis=1, concat_axis=0, tiled=True)
    query_rows = summed_blocks(
        jnp.dot(columns, query_weight, preferred_element_type=jnp.float32), "ep"
    ).astype(jnp.bfloat16)
    query_heads = rms_scale(
        query_rows.astype(jnp.float32).reshape(seq_count, heads_local, DH), query_gain
    ).astype(jnp.bfloat16)
    fresh = jnp.concatenate(
        [
            jnp.dot(columns, key_weight, preferred_element_type=jnp.float32),
            jnp.dot(columns, value_weight, preferred_element_type=jnp.float32),
        ],
        axis=1,
    )
    fresh = summed_blocks(fresh, "ep").astype(jnp.bfloat16)
    new_values = fresh[:, head_cols:]
    new_keys = rms_scale(
        fresh[:, :head_cols].astype(jnp.float32).reshape(seq_count, heads_local, DH), 1.0
    )
    new_keys = new_keys.astype(jnp.bfloat16).reshape(seq_count, head_cols)

    scores = jnp.einsum("shd,shld->shl", query_heads, key_cache, preferred_element_type=jnp.float32)
    scores = scores * DH ** (-0.5) + stick_bias[None, :, None]
    positions = jnp.arange(cache_slots, dtype=jnp.int32)
    visible = positions[None, None, :] < lengths[:, None, None]
    log_rest = jnp.where(visible, jax.nn.log_sigmoid(-scores), 0.0)
    later = (positions[:, None] > positions[None, :]).astype(jnp.float32)
    log_between = jnp.dot(
        log_rest.reshape(-1, cache_slots), later, precision=lax.Precision.HIGHEST
    ).reshape(scores.shape)
    stick = jnp.where(visible, jnp.exp(jax.nn.log_sigmoid(scores) + log_between), 0.0).astype(
        jnp.bfloat16
    )
    attended = jnp.einsum("shl,shld->shd", stick, value_cache, preferred_element_type=jnp.float32)
    attended = attended.astype(jnp.bfloat16).reshape(seq_count, head_cols)
    attn_part = jnp.dot(attended, out_weight, preferred_element_type=jnp.float32)
    attn_parts = lax.all_gather(attn_part.astype(jnp.bfloat16), "tp", axis=0, tiled=False)
    attn_proj = jnp.sum(attn_parts.astype(jnp.float32), axis=0)
    middle = (stream + attn_proj).astype(jnp.bfloat16)
    normed_mix = rms_scale(middle.astype(jnp.float32), mix_gain).astype(jnp.bfloat16)

    top_count = route_ids.shape[1]
    capacity = max(2, 2 * top_count * seq_count // experts)
    slots = experts * capacity
    flat_ids = route_ids.reshape(-1)
    onehot = (flat_ids[:, None] == jnp.arange(experts, dtype=jnp.int32)[None, :]).astype(jnp.int32)
    order = jnp.arange(flat_ids.shape[0], dtype=jnp.int32)
    earlier = (order[:, None] > order[None, :]) & (flat_ids[:, None] == flat_ids[None, :])
    slot_index = jnp.sum(earlier.astype(jnp.int32), axis=1)
    target = flat_ids * capacity + slot_index
    route_map = (target[:, None] == jnp.arange(slots, dtype=jnp.int32)[None, :]).astype(
        jnp.bfloat16
    )
    dispatch = jnp.sum(route_map.reshape(seq_count, top_count, slots), axis=1).T
    outbox = jnp.dot(dispatch, normed_mix, preferred_element_type=jnp.float32).astype(jnp.bfloat16)
    slot_rows = lax.all_to_all(outbox, "ep", split_axis=0, concat_axis=0, tiled=True)

    side_gate_pre = jnp.dot(normed_mix, side_gate, preferred_element_type=jnp.float32)
    side_up_pre = jnp.dot(normed_mix, side_up, preferred_element_type=jnp.float32)
    side_hidden = (jax.nn.silu(side_gate_pre) * side_up_pre).astype(jnp.bfloat16)
    side_term = jnp.dot(side_hidden, side_down, preferred_element_type=jnp.float32)
    switch = jax.nn.sigmoid(
        jnp.sum(normed_mix.astype(jnp.float32) * branch_gate, axis=1, keepdims=True)
    )
    col_width = model_width // tp_size
    col_offset = lax.axis_index("tp") * col_width
    side_blocks = lax.all_to_all(
        side_term.astype(jnp.bfloat16).reshape(seq_count, tp_size, col_width).transpose(1, 0, 2),
        "tp",
        split_axis=0,
        concat_axis=0,
        tiled=True,
    )
    side_part = jnp.sum(side_blocks.astype(jnp.float32), axis=0)

    gate_pre = jnp.dot(slot_rows, expert_gate[0], preferred_element_type=jnp.float32)
    up_pre = jnp.dot(slot_rows, expert_up[0], preferred_element_type=jnp.float32)
    hidden = (jax.nn.silu(gate_pre) * up_pre).astype(jnp.bfloat16)
    expert_term = jnp.dot(hidden, expert_down[0], preferred_element_type=jnp.float32)
    expert_term = expert_term.astype(jnp.bfloat16).reshape(experts, capacity, tp_size, col_width)
    returned = lax.all_to_all(
        expert_term.transpose(0, 2, 1, 3).reshape(experts * tp_size, capacity, col_width),
        ("ep", "tp"),
        split_axis=0,
        concat_axis=0,
        tiled=True,
    )
    expert_out = jnp.sum(
        returned.reshape(experts, tp_size, capacity, col_width).astype(jnp.float32), axis=1
    ).astype(jnp.bfloat16)
    picked = jnp.dot(
        route_map, expert_out.reshape(slots, col_width), preferred_element_type=jnp.float32
    )
    routed = jnp.sum(
        route_weights[:, :, None] * picked.reshape(seq_count, top_count, col_width), axis=1
    )
    middle_cols = lax.dynamic_slice_in_dim(middle, col_offset, col_width, 1).astype(jnp.float32)
    mixed = (middle_cols + routed + switch * side_part).astype(jnp.bfloat16)
    return (mixed, new_keys, new_values)


def solution(mesh):
    in_specs = (
        P("ep", None),
        P(),
        P("ep", "tp"),
        P("ep", "tp"),
        P("ep", "tp"),
        P(),
        P("tp"),
        P("ep", "tp", None, None),
        P("ep", "tp", None, None),
        P("ep"),
        P("tp", None),
        P(),
        P("ep", None),
        P("ep", None),
        P("ep", None, "tp"),
        P("ep", None, "tp"),
        P("ep", "tp", None),
        P(None, "tp"),
        P(None, "tp"),
        P("tp", None),
        P(),
    )
    out_specs = (P("ep", "tp"), P("ep", "tp"), P("ep", "tp"))
    return jax.shard_map(body, mesh=mesh, in_specs=in_specs, out_specs=out_specs, check_vma=False)
```

```python
import jax
import jax.numpy as jnp
from jax import lax
from jax.experimental import pallas as pl
from jax.experimental.pallas import tpu as pltpu
from jax.sharding import PartitionSpec as P


DH = 128
COPY_BYTES = 1 << 20
LANES = 128


epsilon = 1e-06


def rms_scale(values, scale_gain):
    mean_square = jnp.mean(values * values, axis=-1, keepdims=True)
    return values * lax.rsqrt(mean_square + epsilon) * scale_gain


def summed_blocks(partial, axis_name):
    count = lax.axis_size(axis_name)
    rows = partial.shape[0] // count
    blocks = lax.all_to_all(
        partial.astype(jnp.bfloat16), axis_name, split_axis=0, concat_axis=0, tiled=True
    )
    return jnp.sum(blocks.reshape(count, rows, -1).astype(jnp.float32), axis=0)


def plain_layer(
    tokens,
    attn_gain,
    query_weight,
    key_weight,
    value_weight,
    query_gain,
    stick_bias,
    key_cache,
    value_cache,
    lengths,
    out_weight,
    mix_gain,
    route_ids,
    route_weights,
    expert_gate,
    expert_up,
    expert_down,
    side_gate,
    side_up,
    side_down,
    branch_gate,
):
    seq_count, model_width = tokens.shape
    head_cols = query_weight.shape[1]
    heads_local = key_cache.shape[1]
    cache_slots = key_cache.shape[2]
    experts = lax.axis_size("ep")
    tp_size = lax.axis_size("tp")
    stream = tokens.astype(jnp.float32)
    normed = rms_scale(stream, attn_gain).astype(jnp.bfloat16)
    columns = lax.all_to_all(normed, "ep", split_axis=1, concat_axis=0, tiled=True)
    query_rows = summed_blocks(
        jnp.dot(columns, query_weight, preferred_element_type=jnp.float32), "ep"
    ).astype(jnp.bfloat16)
    query_heads = rms_scale(
        query_rows.astype(jnp.float32).reshape(seq_count, heads_local, DH), query_gain
    ).astype(jnp.bfloat16)
    fresh = jnp.concatenate(
        [
            jnp.dot(columns, key_weight, preferred_element_type=jnp.float32),
            jnp.dot(columns, value_weight, preferred_element_type=jnp.float32),
        ],
        axis=1,
    )
    fresh = summed_blocks(fresh, "ep").astype(jnp.bfloat16)
    new_values = fresh[:, head_cols:]
    new_keys = rms_scale(
        fresh[:, :head_cols].astype(jnp.float32).reshape(seq_count, heads_local, DH), 1.0
    )
    new_keys = new_keys.astype(jnp.bfloat16).reshape(seq_count, head_cols)

    scores = jnp.einsum("shd,shld->shl", query_heads, key_cache, preferred_element_type=jnp.float32)
    scores = scores * DH ** (-0.5) + stick_bias[None, :, None]
    positions = jnp.arange(cache_slots, dtype=jnp.int32)
    visible = positions[None, None, :] < lengths[:, None, None]
    log_rest = jnp.where(visible, jax.nn.log_sigmoid(-scores), 0.0)
    later = (positions[:, None] > positions[None, :]).astype(jnp.float32)
    log_between = jnp.dot(
        log_rest.reshape(-1, cache_slots), later, precision=lax.Precision.HIGHEST
    ).reshape(scores.shape)
    stick = jnp.where(visible, jnp.exp(jax.nn.log_sigmoid(scores) + log_between), 0.0).astype(
        jnp.bfloat16
    )
    attended = jnp.einsum("shl,shld->shd", stick, value_cache, preferred_element_type=jnp.float32)
    attended = attended.astype(jnp.bfloat16).reshape(seq_count, head_cols)
    attn_part = jnp.dot(attended, out_weight, preferred_element_type=jnp.float32)
    attn_parts = lax.all_gather(attn_part.astype(jnp.bfloat16), "tp", axis=0, tiled=False)
    attn_proj = jnp.sum(attn_parts.astype(jnp.float32), axis=0)
    middle = (stream + attn_proj).astype(jnp.bfloat16)
    normed_mix = rms_scale(middle.astype(jnp.float32), mix_gain).astype(jnp.bfloat16)

    top_count = route_ids.shape[1]
    capacity = max(2, 2 * top_count * seq_count // experts)
    slots = experts * capacity
    flat_ids = route_ids.reshape(-1)
    onehot = (flat_ids[:, None] == jnp.arange(experts, dtype=jnp.int32)[None, :]).astype(jnp.int32)
    order = jnp.arange(flat_ids.shape[0], dtype=jnp.int32)
    earlier = (order[:, None] > order[None, :]) & (flat_ids[:, None] == flat_ids[None, :])
    slot_index = jnp.sum(earlier.astype(jnp.int32), axis=1)
    target = flat_ids * capacity + slot_index
    route_map = (target[:, None] == jnp.arange(slots, dtype=jnp.int32)[None, :]).astype(
        jnp.bfloat16
    )
    dispatch = jnp.sum(route_map.reshape(seq_count, top_count, slots), axis=1).T
    outbox = jnp.dot(dispatch, normed_mix, preferred_element_type=jnp.float32).astype(jnp.bfloat16)
    slot_rows = lax.all_to_all(outbox, "ep", split_axis=0, concat_axis=0, tiled=True)

    side_gate_pre = jnp.dot(normed_mix, side_gate, preferred_element_type=jnp.float32)
    side_up_pre = jnp.dot(normed_mix, side_up, preferred_element_type=jnp.float32)
    side_hidden = (jax.nn.silu(side_gate_pre) * side_up_pre).astype(jnp.bfloat16)
    side_term = jnp.dot(side_hidden, side_down, preferred_element_type=jnp.float32)
    switch = jax.nn.sigmoid(
        jnp.sum(normed_mix.astype(jnp.float32) * branch_gate, axis=1, keepdims=True)
    )
    col_width = model_width // tp_size
    col_offset = lax.axis_index("tp") * col_width
    side_blocks = lax.all_to_all(
        side_term.astype(jnp.bfloat16).reshape(seq_count, tp_size, col_width).transpose(1, 0, 2),
        "tp",
        split_axis=0,
        concat_axis=0,
        tiled=True,
    )
    side_part = jnp.sum(side_blocks.astype(jnp.float32), axis=0)

    gate_pre = jnp.dot(slot_rows, expert_gate[0], preferred_element_type=jnp.float32)
    up_pre = jnp.dot(slot_rows, expert_up[0], preferred_element_type=jnp.float32)
    hidden = (jax.nn.silu(gate_pre) * up_pre).astype(jnp.bfloat16)
    expert_term = jnp.dot(hidden, expert_down[0], preferred_element_type=jnp.float32)
    expert_term = expert_term.astype(jnp.bfloat16).reshape(experts, capacity, tp_size, col_width)
    returned = lax.all_to_all(
        expert_term.transpose(0, 2, 1, 3).reshape(experts * tp_size, capacity, col_width),
        ("ep", "tp"),
        split_axis=0,
        concat_axis=0,
        tiled=True,
    )
    expert_out = jnp.sum(
        returned.reshape(experts, tp_size, capacity, col_width).astype(jnp.float32), axis=1
    ).astype(jnp.bfloat16)
    picked = jnp.dot(
        route_map, expert_out.reshape(slots, col_width), preferred_element_type=jnp.float32
    )
    routed = jnp.sum(
        route_weights[:, :, None] * picked.reshape(seq_count, top_count, col_width), axis=1
    )
    middle_cols = lax.dynamic_slice_in_dim(middle, col_offset, col_width, 1).astype(jnp.float32)
    mixed = (middle_cols + routed + switch * side_part).astype(jnp.bfloat16)
    return (mixed, new_keys, new_values)


def in_vmem(count):
    return [pl.BlockSpec(memory_space=pltpu.VMEM)] * count


def call(kernel, outs, *arrays, scalars=0, limit=8 << 20):
    return pl.pallas_call(
        kernel,
        out_shape=[jax.ShapeDtypeStruct(shape, dtype) for shape, dtype in outs],
        in_specs=[pl.BlockSpec(memory_space=pltpu.SMEM)] * scalars
        + in_vmem(len(arrays) - scalars),
        out_specs=in_vmem(len(outs)),
        compiler_params=pltpu.CompilerParams(vmem_limit_bytes=limit),
    )(*arrays)


def stage(*groups):
    plan, shapes = [], []
    for target, group in enumerate(groups):
        offset = 0
        for array in group:
            size = array.size * array.dtype.itemsize
            count = max(1, size // COPY_BYTES)
            while array.shape[0] % count:
                count -= 1
            plan.append((target, offset, array.shape[0] // count, count))
            offset += array.shape[0]
        shapes.append(pltpu.VMEM((offset,) + group[0].shape[1:], group[0].dtype))
    arrays = [array for group in groups for array in group]
    total = sum(count for *_, count in plan)

    def kernel(*refs):
        sources, targets, sems = refs[: len(arrays)], refs[len(arrays) : -1], refs[-1]
        copies = []
        for source, (target, offset, rows, count) in zip(sources, plan):
            for i in range(count):
                copies.append(
                    pltpu.make_async_copy(
                        source.at[pl.ds(i * rows, rows)],
                        targets[target].at[pl.ds(offset + i * rows, rows)],
                        sems.at[len(copies)],
                    )
                )
        for copy in copies:
            copy.start()
        for copy in copies:
            copy.wait()

    return pl.pallas_call(
        kernel,
        out_shape=shapes,
        in_specs=[pl.BlockSpec(memory_space=pltpu.HBM) for _ in arrays],
        out_specs=in_vmem(len(groups)),
        scratch_shapes=[pltpu.SemaphoreType.DMA((total,))],
        compiler_params=pltpu.CompilerParams(vmem_limit_bytes=1 << 20),
    )(*[pltpu.with_memory_space_constraint(array, pltpu.HBM) for array in arrays])


def place():
    index = lax.axis_index("ep")
    return lax.div(index, jnp.int32(2)), lax.rem(index, jnp.int32(2))


def pair_move(values):
    count = lax.axis_size("ep")
    return lax.ppermute(values, "ep", [(i, i ^ 1) for i in range(count)])


def far_move(values, step):
    count = lax.axis_size("ep")
    return lax.ppermute(values, "ep", [(i, i ^ (2 * step)) for i in range(count)])


def tp_move(values, turn):
    count = lax.axis_size("tp")
    return lax.ppermute(values, "tp", [(i, i ^ turn) for i in range(count)])


def aligned(index, size):
    return pl.multiple_of(index * size, size)


def split_tokens(tokens):
    rows, width = tokens.shape
    count = lax.axis_size("ep")
    features = width // count
    half = count // 2

    def kernel(tokens_ref, away_ref, kept_ref, scale_ref):
        high, low = place()
        for step in range(half):
            for target, side in ((kept_ref, low), (away_ref, 1 - low)):
                column = aligned(2 * (high ^ step) + side, features)
                target[step] = tokens_ref[:, pl.ds(column, features)]
        stream = tokens_ref[...].astype(jnp.float32)
        mean_square = jnp.mean(stream * stream, axis=-1, keepdims=True)
        scale_ref[...] = jnp.broadcast_to(lax.rsqrt(mean_square + epsilon), scale_ref.shape)

    shape = (half, rows, features)
    return call(
        kernel,
        [(shape, tokens.dtype), (shape, tokens.dtype), ((rows, LANES), jnp.float32)],
        tokens,
    )


def knit(kept, came):
    half, rows, width = kept.shape

    def kernel(kept_ref, came_ref, *outs):
        for step, out_ref in enumerate(outs):
            out_ref[...] = jnp.concatenate([kept_ref[step], came_ref[step]], axis=0)

    return call(kernel, [((2 * rows, width), kept.dtype)] * half, kept, came)


def project(parts, gain, weights, parts_out):
    features = parts[0].shape[1]
    rows = parts[0].shape[0] // 2
    half = len(parts)
    wide = weights.shape[1]

    def kernel(*refs):
        part_refs, (gain_ref, weight_ref, away_ref, kept_ref) = refs[:half], refs[half:]
        gain_part = gain_ref[:, pl.ds(aligned(lax.axis_index("ep"), features), features)]
        values = [ref[...].astype(jnp.float32) for ref in part_refs]
        ordered = [value[rows:] for value in values] + [value[:rows] for value in values]
        lines = (jnp.concatenate(ordered, axis=0) * gain_part).astype(jnp.bfloat16)
        for i in range(parts_out):
            weight = weight_ref[i * features : (i + 1) * features, :]
            part = jnp.dot(lines, weight, preferred_element_type=jnp.float32)
            away_ref[:, i * wide : (i + 1) * wide] = part[: half * rows].astype(jnp.bfloat16)
            kept_ref[:, i * wide : (i + 1) * wide] = part[half * rows :]

    shape = (half * rows, parts_out * wide)
    return call(
        kernel,
        [(shape, jnp.bfloat16), (shape, jnp.float32)],
        *parts,
        gain.reshape(1, -1),
        weights,
        limit=16 << 20,
    )


def slots_of(ids_ref):
    chosen = []
    for b in range(ids_ref.shape[1]):
        for k in range(ids_ref.shape[0]):
            expert = ids_ref[k, b]
            slot = jnp.int32(0)
            for _, _, other, _ in chosen:
                slot = slot + (other == expert).astype(jnp.int32)
            chosen.append((b, k, expert, slot))
    return chosen


def dispatch(ids, weights, tokens, attn_parts, mix_gain, capacity):
    rows, width = tokens.shape
    count, tp_size = lax.axis_size("ep"), lax.axis_size("tp")
    half = count // 2
    col_width = width // tp_size
    slots = half * capacity
    terms = len(attn_parts)

    def kernel(ids_ref, weights_ref, tokens_ref, *refs):
        part_refs, gain_ref = refs[:terms], refs[terms]
        middle_ref, kept_ref, away_ref, scratch = refs[terms + 1 :]
        proj = part_refs[0][...].astype(jnp.float32)
        for ref in part_refs[1:]:
            proj = proj + ref[...].astype(jnp.float32)
        middle = (tokens_ref[...].astype(jnp.float32) + proj).astype(jnp.bfloat16)
        wide = middle.astype(jnp.float32)
        scratch[...] = wide
        column = aligned(lax.axis_index("tp"), col_width)
        middle_ref[...] = scratch[:, pl.ds(column, col_width)]
        mean_square = jnp.mean(wide * wide, axis=-1, keepdims=True)
        normed = (wide * lax.rsqrt(mean_square + epsilon) * gain_ref[...]).astype(jnp.bfloat16)
        high, low = place()
        line = lax.broadcasted_iota(jnp.int32, (2 * slots, LANES), 0)
        lane = lax.broadcasted_iota(jnp.int32, (2 * slots, LANES), 1)
        picks = jnp.zeros((2 * slots, LANES), jnp.float32)
        share = jnp.zeros((2 * slots, LANES), jnp.float32)
        first = jnp.zeros((2 * slots, LANES), jnp.float32)
        for b, k, expert, slot in slots_of(ids_ref):
            block = lax.div(expert, jnp.int32(2)) ^ high
            side = lax.rem(expert, jnp.int32(2)) ^ low
            here = line == side * slots + block * capacity + slot
            picks = jnp.where(here & (lane == b), 1.0, picks)
            share = jnp.where(here, weights_ref[k, b], share)
            if k == 0:
                first = jnp.where(here, 1.0, first)
        outbox = jnp.dot(
            picks[:, :rows].astype(jnp.bfloat16), normed, preferred_element_type=jnp.float32
        ).astype(jnp.bfloat16)
        upper = share.astype(jnp.bfloat16).astype(jnp.float32)
        notes = jnp.where(lane == 0, upper, jnp.where(lane == 1, share - upper, first))
        notes = notes.astype(jnp.bfloat16)
        kept_ref[:, :width] = outbox[:slots]
        away_ref[:, :width] = outbox[slots:]
        kept_ref[:, width:] = notes[:slots]
        away_ref[:, width:] = notes[slots:]

    shape = (slots, width + LANES)
    return pl.pallas_call(
        kernel,
        out_shape=[
            jax.ShapeDtypeStruct((rows, col_width), jnp.float32),
            jax.ShapeDtypeStruct(shape, jnp.bfloat16),
            jax.ShapeDtypeStruct(shape, jnp.bfloat16),
        ],
        in_specs=[pl.BlockSpec(memory_space=pltpu.SMEM)] * 2 + in_vmem(terms + 2),
        out_specs=in_vmem(3),
        scratch_shapes=[pltpu.VMEM((rows, width), jnp.float32)],
        compiler_params=pltpu.CompilerParams(vmem_limit_bytes=8 << 20),
    )(ids, weights, tokens, *attn_parts, mix_gain.reshape(1, -1))


def experts_apply(parts, gate_up, down, side_in, side_back, branch_gate, capacity):
    count, tp_size = lax.axis_size("ep"), lax.axis_size("tp")
    width = parts[0].shape[1] - LANES
    col_width = width // tp_size
    chunks = col_width // LANES

    def kernel(*refs):
        part_refs = refs[: len(parts)]
        gate_up_ref, down_ref, side_in_ref, side_back_ref, branch_ref, out_ref = refs[len(parts) :]
        whole = jnp.concatenate([ref[...] for ref in part_refs], axis=0)
        lines = whole[:, :width]
        notes = whole[:, width:].astype(jnp.float32)
        share = notes[:, 0:1] + notes[:, 1:2]
        logit = jnp.sum(lines.astype(jnp.float32) * branch_ref[...], axis=1, keepdims=True)
        switch = notes[:, 2:3] * jax.nn.sigmoid(logit)

        def hidden_of(ref):
            gate_pre = jnp.dot(lines, ref[:width, :], preferred_element_type=jnp.float32)
            up_pre = jnp.dot(lines, ref[width:, :], preferred_element_type=jnp.float32)
            return (jax.nn.silu(gate_pre) * up_pre).astype(jnp.bfloat16)

        hidden = hidden_of(gate_up_ref)
        side_hidden = hidden_of(side_in_ref)
        high, low = place()
        for t in range(tp_size):
            columns = slice(t * col_width, (t + 1) * col_width)
            result = share * jnp.dot(
                hidden, down_ref[:, columns], preferred_element_type=jnp.float32
            ) + switch * jnp.dot(
                side_hidden, side_back_ref[:, columns], preferred_element_type=jnp.float32
            )
            for step in range(count // 2):
                for part in range(2):
                    source = 2 * (high ^ step) + (low ^ part)
                    start = (2 * step + part) * capacity
                    block = jnp.concatenate(
                        [
                            result[start : start + capacity, c * LANES : (c + 1) * LANES]
                            for c in range(chunks)
                        ],
                        axis=0,
                    )
                    out_ref[source * tp_size + t] = block.astype(jnp.bfloat16)

    shape = (count * tp_size, chunks * capacity, LANES)
    return call(
        kernel,
        [(shape, jnp.bfloat16)],
        *parts,
        gate_up,
        down,
        side_in,
        side_back,
        branch_gate.reshape(1, -1),
        limit=12 << 20,
    )[0]


def home_picks(ids, rows, capacity, chunks):
    count, tp_size = lax.axis_size("ep"), lax.axis_size("tp")
    per_block = chunks * capacity
    total = count * tp_size * per_block

    def kernel(ids_ref, out_ref):
        row = lax.broadcasted_iota(jnp.int32, (chunks * rows, total), 0)
        column = lax.broadcasted_iota(jnp.int32, (chunks * rows, total), 1)
        expert_of = lax.div(column, jnp.int32(tp_size * per_block))
        within = lax.rem(column, jnp.int32(per_block))
        same = lax.div(within, jnp.int32(capacity)) == lax.div(row, jnp.int32(rows))
        key = expert_of * capacity + lax.rem(within, jnp.int32(capacity))
        token = lax.rem(row, jnp.int32(rows))
        picks = jnp.zeros((chunks * rows, total), jnp.float32)
        for b, _, expert, slot in slots_of(ids_ref):
            hit = (key == expert * capacity + slot) & (token == b)
            picks = jnp.where(hit, 1.0, picks)
        out_ref[...] = jnp.where(same, picks, 0.0).astype(jnp.bfloat16)

    shape = (chunks * rows, total)
    return call(kernel, [(shape, jnp.bfloat16)], ids, scalars=1)[0]


def finish(picks, returned, middle):
    rows, col_width = middle.shape
    chunks = col_width // LANES

    def kernel(picks_ref, returned_ref, middle_ref, out_ref):
        lines = returned_ref[...].reshape(-1, LANES)
        sums = jnp.dot(picks_ref[...], lines, preferred_element_type=jnp.float32)
        for c in range(chunks):
            columns = slice(c * LANES, (c + 1) * LANES)
            total = middle_ref[:, columns] + sums[c * rows : (c + 1) * rows]
            out_ref[:, columns] = total.astype(jnp.bfloat16)

    return call(kernel, [((rows, col_width), jnp.bfloat16)], picks, returned, middle)[0]


def fast_layer(
    tokens,
    attn_gain,
    query_weight,
    key_weight,
    value_weight,
    query_gain,
    stick_bias,
    key_cache,
    value_cache,
    lengths,
    out_weight,
    mix_gain,
    route_ids,
    route_weights,
    expert_gate,
    expert_up,
    expert_down,
    side_gate,
    side_up,
    side_down,
    branch_gate,
):
    seq_count, model_width = tokens.shape
    head_cols = query_weight.shape[1]
    heads_local = key_cache.shape[1]
    cache_slots = key_cache.shape[2]
    experts, tp_size = lax.axis_size("ep"), lax.axis_size("tp")
    half = experts // 2
    top_count = route_ids.shape[1]
    capacity = max(2, 2 * top_count * seq_count // experts)

    away, kept, scales = split_tokens(tokens)
    came = pair_move(away)
    parts = knit(kept, came)
    parts = [parts[0]] + [far_move(parts[step], step) for step in range(1, half)]
    key_cache, weights = stage([key_cache], [query_weight, key_weight, value_weight])
    away, kept = project(parts, attn_gain, weights, 3)
    came = pair_move(away)
    both = kept + came.astype(jnp.float32)
    projected = both[:seq_count]
    for step in range(1, half):
        leaving = both[step * seq_count : (step + 1) * seq_count].astype(jnp.bfloat16)
        moved = far_move(leaving, step)
        projected = projected + moved.astype(jnp.float32)
    projected = (projected * scales[:, :1]).astype(jnp.bfloat16)
    query_rows = projected[:, :head_cols]
    fresh_keys = projected[:, head_cols : 2 * head_cols].astype(jnp.float32)
    new_values = projected[:, 2 * head_cols :]
    new_keys = rms_scale(fresh_keys.reshape(seq_count, heads_local, DH), 1.0)
    new_keys = new_keys.astype(jnp.bfloat16).reshape(seq_count, head_cols)
    query_heads = rms_scale(
        query_rows.astype(jnp.float32).reshape(seq_count, heads_local, DH), query_gain
    ).astype(jnp.bfloat16)
    value_cache, out_weight = stage([value_cache], [out_weight])

    scores = jnp.einsum("shd,shld->shl", query_heads, key_cache, preferred_element_type=jnp.float32)
    scores = scores * DH ** (-0.5) + stick_bias[None, :, None]
    positions = jnp.arange(cache_slots, dtype=jnp.int32)
    visible = positions[None, None, :] < lengths[:, None, None]
    log_rest = jnp.where(visible, jax.nn.log_sigmoid(-scores), 0.0)
    later = (positions[:, None] > positions[None, :]).astype(jnp.float32)
    log_between = jnp.dot(
        log_rest.reshape(-1, cache_slots), later, precision=lax.Precision.HIGHEST
    ).reshape(scores.shape)
    stick = jnp.where(visible, jnp.exp(jax.nn.log_sigmoid(scores) + log_between), 0.0).astype(
        jnp.bfloat16
    )
    attended = jnp.einsum("shl,shld->shd", stick, value_cache, preferred_element_type=jnp.float32)
    attended = attended.astype(jnp.bfloat16).reshape(seq_count, head_cols)
    attn_part = jnp.dot(attended, out_weight, preferred_element_type=jnp.float32)
    attn_part = attn_part.astype(jnp.bfloat16)
    attn_parts = [attn_part] + [tp_move(attn_part, turn) for turn in range(1, tp_size)]
    side_in, side_back = stage([side_gate, side_up], [side_down])

    ids, weights_t = route_ids.T, route_weights.T
    middle, kept, away = dispatch(ids, weights_t, tokens, attn_parts, mix_gain, capacity)
    came = pair_move(away)
    kept = kept.reshape(half, capacity, -1)
    came = came.reshape(half, capacity, -1)
    parts = [jnp.concatenate([kept[step], came[step]], axis=0) for step in range(half)]
    parts = [parts[0]] + [far_move(parts[step], step) for step in range(1, half)]
    (gate_up,) = stage([expert_gate[0], expert_up[0]])
    blocks = experts_apply(
        parts, gate_up, expert_down[0], side_in, side_back, branch_gate, capacity
    )
    returned = lax.all_to_all(
        blocks, ("ep", "tp"), split_axis=0, concat_axis=0, tiled=True
    )
    picks = home_picks(ids, seq_count, capacity, model_width // tp_size // LANES)
    mixed = finish(picks, returned, middle)
    return (mixed, new_keys, new_values)


def two_power(count):
    return count & (count - 1) == 0


def body(*arrays):
    tokens = arrays[0]
    experts, tp_size = lax.axis_size("ep"), lax.axis_size("tp")
    widths = (tokens.shape[1] // experts, tokens.shape[1] // tp_size, arrays[14].shape[2])
    fits = experts > 1 and two_power(experts) and two_power(tp_size)
    fits = fits and all(width % LANES == 0 for width in widths)
    fits = fits and tokens.shape[0] == 8
    return (fast_layer if fits else plain_layer)(*arrays)


def solution(mesh):
    in_specs = (
        P("ep", None),
        P(),
        P("ep", "tp"),
        P("ep", "tp"),
        P("ep", "tp"),
        P(),
        P("tp"),
        P("ep", "tp", None, None),
        P("ep", "tp", None, None),
        P("ep"),
        P("tp", None),
        P(),
        P("ep", None),
        P("ep", None),
        P("ep", None, "tp"),
        P("ep", None, "tp"),
        P("ep", "tp", None),
        P(None, "tp"),
        P(None, "tp"),
        P("tp", None),
        P(),
    )
    out_specs = (P("ep", "tp"), P("ep", "tp"), P("ep", "tp"))
    return jax.shard_map(body, mesh=mesh, in_specs=in_specs, out_specs=out_specs, check_vma=False)
```

```python
import jax
import jax.numpy as jnp
from jax import lax
from jax.experimental import pallas as pl
from jax.experimental.pallas import tpu as pltpu
from jax.sharding import PartitionSpec as P


DH = 128
COPY_BYTES = 1 << 20
LANES = 128


epsilon = 1e-06


def rms_scale(values, scale_gain):
    mean_square = jnp.mean(values * values, axis=-1, keepdims=True)
    return values * lax.rsqrt(mean_square + epsilon) * scale_gain


def summed_blocks(partial, axis_name):
    count = lax.axis_size(axis_name)
    rows = partial.shape[0] // count
    blocks = lax.all_to_all(
        partial.astype(jnp.bfloat16), axis_name, split_axis=0, concat_axis=0, tiled=True
    )
    return jnp.sum(blocks.reshape(count, rows, -1).astype(jnp.float32), axis=0)


def plain_layer(
    tokens,
    attn_gain,
    query_weight,
    key_weight,
    value_weight,
    query_gain,
    stick_bias,
    key_cache,
    value_cache,
    lengths,
    out_weight,
    mix_gain,
    route_ids,
    route_weights,
    expert_gate,
    expert_up,
    expert_down,
    side_gate,
    side_up,
    side_down,
    branch_gate,
):
    seq_count, model_width = tokens.shape
    head_cols = query_weight.shape[1]
    heads_local = key_cache.shape[1]
    cache_slots = key_cache.shape[2]
    experts = lax.axis_size("ep")
    tp_size = lax.axis_size("tp")
    stream = tokens.astype(jnp.float32)
    normed = rms_scale(stream, attn_gain).astype(jnp.bfloat16)
    columns = lax.all_to_all(normed, "ep", split_axis=1, concat_axis=0, tiled=True)
    query_rows = summed_blocks(
        jnp.dot(columns, query_weight, preferred_element_type=jnp.float32), "ep"
    ).astype(jnp.bfloat16)
    query_heads = rms_scale(
        query_rows.astype(jnp.float32).reshape(seq_count, heads_local, DH), query_gain
    ).astype(jnp.bfloat16)
    fresh = jnp.concatenate(
        [
            jnp.dot(columns, key_weight, preferred_element_type=jnp.float32),
            jnp.dot(columns, value_weight, preferred_element_type=jnp.float32),
        ],
        axis=1,
    )
    fresh = summed_blocks(fresh, "ep").astype(jnp.bfloat16)
    new_values = fresh[:, head_cols:]
    new_keys = rms_scale(
        fresh[:, :head_cols].astype(jnp.float32).reshape(seq_count, heads_local, DH), 1.0
    )
    new_keys = new_keys.astype(jnp.bfloat16).reshape(seq_count, head_cols)

    scores = jnp.einsum("shd,shld->shl", query_heads, key_cache, preferred_element_type=jnp.float32)
    scores = scores * DH ** (-0.5) + stick_bias[None, :, None]
    positions = jnp.arange(cache_slots, dtype=jnp.int32)
    visible = positions[None, None, :] < lengths[:, None, None]
    log_rest = jnp.where(visible, jax.nn.log_sigmoid(-scores), 0.0)
    later = (positions[:, None] > positions[None, :]).astype(jnp.float32)
    log_between = jnp.dot(
        log_rest.reshape(-1, cache_slots), later, precision=lax.Precision.HIGHEST
    ).reshape(scores.shape)
    stick = jnp.where(visible, jnp.exp(jax.nn.log_sigmoid(scores) + log_between), 0.0).astype(
        jnp.bfloat16
    )
    attended = jnp.einsum("shl,shld->shd", stick, value_cache, preferred_element_type=jnp.float32)
    attended = attended.astype(jnp.bfloat16).reshape(seq_count, head_cols)
    attn_part = jnp.dot(attended, out_weight, preferred_element_type=jnp.float32)
    attn_parts = lax.all_gather(attn_part.astype(jnp.bfloat16), "tp", axis=0, tiled=False)
    attn_proj = jnp.sum(attn_parts.astype(jnp.float32), axis=0)
    middle = (stream + attn_proj).astype(jnp.bfloat16)
    normed_mix = rms_scale(middle.astype(jnp.float32), mix_gain).astype(jnp.bfloat16)

    top_count = route_ids.shape[1]
    capacity = max(2, 2 * top_count * seq_count // experts)
    slots = experts * capacity
    flat_ids = route_ids.reshape(-1)
    onehot = (flat_ids[:, None] == jnp.arange(experts, dtype=jnp.int32)[None, :]).astype(jnp.int32)
    order = jnp.arange(flat_ids.shape[0], dtype=jnp.int32)
    earlier = (order[:, None] > order[None, :]) & (flat_ids[:, None] == flat_ids[None, :])
    slot_index = jnp.sum(earlier.astype(jnp.int32), axis=1)
    target = flat_ids * capacity + slot_index
    route_map = (target[:, None] == jnp.arange(slots, dtype=jnp.int32)[None, :]).astype(
        jnp.bfloat16
    )
    dispatch = jnp.sum(route_map.reshape(seq_count, top_count, slots), axis=1).T
    outbox = jnp.dot(dispatch, normed_mix, preferred_element_type=jnp.float32).astype(jnp.bfloat16)
    slot_rows = lax.all_to_all(outbox, "ep", split_axis=0, concat_axis=0, tiled=True)

    side_gate_pre = jnp.dot(normed_mix, side_gate, preferred_element_type=jnp.float32)
    side_up_pre = jnp.dot(normed_mix, side_up, preferred_element_type=jnp.float32)
    side_hidden = (jax.nn.silu(side_gate_pre) * side_up_pre).astype(jnp.bfloat16)
    side_term = jnp.dot(side_hidden, side_down, preferred_element_type=jnp.float32)
    switch = jax.nn.sigmoid(
        jnp.sum(normed_mix.astype(jnp.float32) * branch_gate, axis=1, keepdims=True)
    )
    col_width = model_width // tp_size
    col_offset = lax.axis_index("tp") * col_width
    side_blocks = lax.all_to_all(
        side_term.astype(jnp.bfloat16).reshape(seq_count, tp_size, col_width).transpose(1, 0, 2),
        "tp",
        split_axis=0,
        concat_axis=0,
        tiled=True,
    )
    side_part = jnp.sum(side_blocks.astype(jnp.float32), axis=0)

    gate_pre = jnp.dot(slot_rows, expert_gate[0], preferred_element_type=jnp.float32)
    up_pre = jnp.dot(slot_rows, expert_up[0], preferred_element_type=jnp.float32)
    hidden = (jax.nn.silu(gate_pre) * up_pre).astype(jnp.bfloat16)
    expert_term = jnp.dot(hidden, expert_down[0], preferred_element_type=jnp.float32)
    expert_term = expert_term.astype(jnp.bfloat16).reshape(experts, capacity, tp_size, col_width)
    returned = lax.all_to_all(
        expert_term.transpose(0, 2, 1, 3).reshape(experts * tp_size, capacity, col_width),
        ("ep", "tp"),
        split_axis=0,
        concat_axis=0,
        tiled=True,
    )
    expert_out = jnp.sum(
        returned.reshape(experts, tp_size, capacity, col_width).astype(jnp.float32), axis=1
    ).astype(jnp.bfloat16)
    picked = jnp.dot(
        route_map, expert_out.reshape(slots, col_width), preferred_element_type=jnp.float32
    )
    routed = jnp.sum(
        route_weights[:, :, None] * picked.reshape(seq_count, top_count, col_width), axis=1
    )
    middle_cols = lax.dynamic_slice_in_dim(middle, col_offset, col_width, 1).astype(jnp.float32)
    mixed = (middle_cols + routed + switch * side_part).astype(jnp.bfloat16)
    return (mixed, new_keys, new_values)


def in_vmem(count):
    return [pl.BlockSpec(memory_space=pltpu.VMEM)] * count


def call(kernel, outs, *arrays, scalars=0, limit=8 << 20):
    return pl.pallas_call(
        kernel,
        out_shape=[jax.ShapeDtypeStruct(shape, dtype) for shape, dtype in outs],
        in_specs=[pl.BlockSpec(memory_space=pltpu.SMEM)] * scalars
        + in_vmem(len(arrays) - scalars),
        out_specs=in_vmem(len(outs)),
        compiler_params=pltpu.CompilerParams(vmem_limit_bytes=limit),
    )(*arrays)


def stage(*groups, scalars=(), outs=(), work=None):
    plan, shapes = [], []
    for target, group in enumerate(groups):
        offset = 0
        for array in group:
            size = array.size * array.dtype.itemsize
            count = max(1, size // COPY_BYTES)
            while array.shape[0] % count:
                count -= 1
            plan.append((target, offset, array.shape[0] // count, count))
            offset += array.shape[0]
        shapes.append(pltpu.VMEM((offset,) + group[0].shape[1:], group[0].dtype))
    arrays = [array for group in groups for array in group]
    total = sum(count for *_, count in plan)

    def kernel(*refs):
        scalar_refs, refs = refs[: len(scalars)], refs[len(scalars) :]
        sources, sems = refs[: len(arrays)], refs[-1]
        targets = refs[len(arrays) : len(arrays) + len(groups)]
        copies = []
        for source, (target, offset, rows, count) in zip(sources, plan):
            for i in range(count):
                copies.append(
                    pltpu.make_async_copy(
                        source.at[pl.ds(i * rows, rows)],
                        targets[target].at[pl.ds(offset + i * rows, rows)],
                        sems.at[len(copies)],
                    )
                )
        for copy in copies:
            copy.start()
        if work is not None:
            work(*scalar_refs, *refs[len(arrays) + len(groups) : -1])
        for copy in copies:
            copy.wait()

    return pl.pallas_call(
        kernel,
        out_shape=shapes + [jax.ShapeDtypeStruct(shape, dtype) for shape, dtype in outs],
        in_specs=[pl.BlockSpec(memory_space=pltpu.SMEM)] * len(scalars)
        + [pl.BlockSpec(memory_space=pltpu.HBM) for _ in arrays],
        out_specs=in_vmem(len(groups) + len(outs)),
        scratch_shapes=[pltpu.SemaphoreType.DMA((total,))],
        compiler_params=pltpu.CompilerParams(vmem_limit_bytes=1 << 20),
    )(*scalars, *[pltpu.with_memory_space_constraint(array, pltpu.HBM) for array in arrays])


def stage_keys(keys, *arrays):
    seqs, heads, slots, size = keys.shape
    rows = [array.shape[0] for array in arrays]

    def kernel(keys_ref, *refs):
        array_refs = refs[: len(arrays)]
        turned_ref, stacked_ref, scratch, key_sems, array_sems = refs[len(arrays) :]
        key_copies = [
            pltpu.make_async_copy(keys_ref.at[s], scratch.at[s], key_sems.at[s])
            for s in range(seqs)
        ]
        array_copies = [
            pltpu.make_async_copy(
                ref, stacked_ref.at[pl.ds(sum(rows[:i]), rows[i])], array_sems.at[i]
            )
            for i, ref in enumerate(array_refs)
        ]
        for copy in key_copies + array_copies:
            copy.start()
        for s in range(seqs):
            key_copies[s].wait()
            for h in range(heads):
                turned_ref[s, h] = scratch[s, h].T
        for copy in array_copies:
            copy.wait()

    return pl.pallas_call(
        kernel,
        out_shape=[
            pltpu.VMEM((seqs, heads, size, slots), keys.dtype),
            pltpu.VMEM((sum(rows),) + arrays[0].shape[1:], arrays[0].dtype),
        ],
        in_specs=[pl.BlockSpec(memory_space=pltpu.HBM)] * (1 + len(arrays)),
        out_specs=in_vmem(2),
        scratch_shapes=[
            pltpu.VMEM(keys.shape, keys.dtype),
            pltpu.SemaphoreType.DMA((seqs,)),
            pltpu.SemaphoreType.DMA((len(arrays),)),
        ],
        compiler_params=pltpu.CompilerParams(vmem_limit_bytes=16 << 20),
    )(*[pltpu.with_memory_space_constraint(array, pltpu.HBM) for array in (keys, *arrays)])


def stage_beside(*pairs):
    def kernel(*refs):
        sources, targets, sems = refs[: 2 * len(pairs)], refs[2 * len(pairs) : -1], refs[-1]
        copies = []
        for n, target in enumerate(targets):
            rows, width = sources[2 * n].shape
            pieces = 4 if rows % 64 == 0 else 1
            for k in range(2):
                for i in range(pieces):
                    part = pl.ds(i * (rows // pieces), rows // pieces)
                    copies.append(
                        pltpu.make_async_copy(
                            sources[2 * n + k].at[part],
                            target.at[part, pl.ds(k * width, width)],
                            sems.at[len(copies)],
                        )
                    )
        for copy in copies:
            copy.start()
        for copy in copies:
            copy.wait()

    arrays = [array for pair in pairs for array in pair]
    return pl.pallas_call(
        kernel,
        out_shape=[
            pltpu.VMEM((pair[0].shape[0], 2 * pair[0].shape[1]), pair[0].dtype) for pair in pairs
        ],
        in_specs=[pl.BlockSpec(memory_space=pltpu.HBM)] * len(arrays),
        out_specs=in_vmem(len(pairs)),
        scratch_shapes=[pltpu.SemaphoreType.DMA((8 * len(pairs),))],
        compiler_params=pltpu.CompilerParams(vmem_limit_bytes=1 << 20),
    )(*[pltpu.with_memory_space_constraint(array, pltpu.HBM) for array in arrays])


def place():
    index = lax.axis_index("ep")
    return lax.div(index, jnp.int32(2)), lax.rem(index, jnp.int32(2))


def pair_move(values):
    count = lax.axis_size("ep")
    return lax.ppermute(values, "ep", [(i, i ^ 1) for i in range(count)])


def far_move(values, step):
    count = lax.axis_size("ep")
    return lax.ppermute(values, "ep", [(i, i ^ (2 * step)) for i in range(count)])


def tp_move(values, turn):
    count = lax.axis_size("tp")
    return lax.ppermute(values, "tp", [(i, i ^ turn) for i in range(count)])


def aligned(index, size):
    return pl.multiple_of(index * size, size)


def row_scales(tokens):
    def kernel(tokens_ref, scale_ref):
        stream = tokens_ref[...].astype(jnp.float32)
        mean_square = jnp.mean(stream * stream, axis=-1, keepdims=True)
        scale_ref[...] = jnp.broadcast_to(lax.rsqrt(mean_square + epsilon), scale_ref.shape)

    return call(kernel, [((tokens.shape[0], LANES), jnp.float32)], tokens)[0]


def knit(tokens, came):
    rows, width = tokens.shape
    count = lax.axis_size("ep")
    features = width // count
    half = count // 2

    def kernel(tokens_ref, came_ref, *outs):
        high, low = place()
        for step, out_ref in enumerate(outs):
            part = pl.ds(aligned(2 * (high ^ step) + low, features), features)
            out_ref[...] = jnp.concatenate([tokens_ref[:, part], came_ref[:, part]], axis=0)

    return call(kernel, [((2 * rows, features), tokens.dtype)] * half, tokens, came)


def project(parts, gain, weights, parts_out):
    features = parts[0].shape[1]
    rows = parts[0].shape[0] // 2
    half = len(parts)
    wide = weights.shape[1]

    def kernel(*refs):
        part_refs, (gain_ref, weight_ref, away_ref, kept_ref) = refs[:half], refs[half:]
        gain_part = gain_ref[:, pl.ds(aligned(lax.axis_index("ep"), features), features)]
        values = [ref[...].astype(jnp.float32) for ref in part_refs]
        ordered = [value[rows:] for value in values] + [value[:rows] for value in values]
        lines = (jnp.concatenate(ordered, axis=0) * gain_part).astype(jnp.bfloat16)
        for i in range(parts_out):
            weight = weight_ref[i * features : (i + 1) * features, :]
            part = jnp.dot(lines, weight, preferred_element_type=jnp.float32)
            away_ref[:, i * wide : (i + 1) * wide] = part[: half * rows].astype(jnp.bfloat16)
            kept_ref[:, i * wide : (i + 1) * wide] = part[half * rows :]

    shape = (half * rows, parts_out * wide)
    return call(
        kernel,
        [(shape, jnp.bfloat16), (shape, jnp.float32)],
        *parts,
        gain.reshape(1, -1),
        weights,
        limit=16 << 20,
    )


def slots_of(ids_ref):
    chosen = []
    for b in range(ids_ref.shape[1]):
        for k in range(ids_ref.shape[0]):
            expert = ids_ref[k, b]
            slot = jnp.int32(0)
            for _, _, other, _ in chosen:
                slot = slot + (other == expert).astype(jnp.int32)
            chosen.append((b, k, expert, slot))
    return chosen


def plan_sends(capacity):
    half = lax.axis_size("ep") // 2
    slots = half * capacity

    def kernel(ids_ref, weights_ref, picks_ref, notes_ref):
        high, low = place()
        line = lax.broadcasted_iota(jnp.int32, (2 * slots, LANES), 0)
        lane = lax.broadcasted_iota(jnp.int32, (2 * slots, LANES), 1)
        picks = jnp.zeros((2 * slots, LANES), jnp.float32)
        share = jnp.zeros((2 * slots, LANES), jnp.float32)
        first = jnp.zeros((2 * slots, LANES), jnp.float32)
        for b, k, expert, slot in slots_of(ids_ref):
            block = lax.div(expert, jnp.int32(2)) ^ high
            side = lax.rem(expert, jnp.int32(2)) ^ low
            here = line == side * slots + block * capacity + slot
            picks = jnp.where(here & (lane == b), 1.0, picks)
            share = jnp.where(here, weights_ref[k, b], share)
            if k == 0:
                first = jnp.where(here, 1.0, first)
        upper = share.astype(jnp.bfloat16).astype(jnp.float32)
        notes = jnp.where(lane == 0, upper, jnp.where(lane == 1, share - upper, first))
        picks_ref[...] = picks.astype(jnp.bfloat16)
        notes_ref[...] = notes.astype(jnp.bfloat16)

    shape = (2 * slots, LANES)
    return [(shape, jnp.bfloat16), (shape, jnp.bfloat16)], kernel


def dispatch(picks, notes, tokens, attn_parts, mix_gain):
    rows, width = tokens.shape
    col_width = width // lax.axis_size("tp")
    slots = picks.shape[0] // 2
    terms = len(attn_parts)

    def kernel(picks_ref, notes_ref, tokens_ref, *refs):
        part_refs, gain_ref = refs[:terms], refs[terms]
        middle_ref, kept_ref, away_ref, scratch = refs[terms + 1 :]
        proj = part_refs[0][...].astype(jnp.float32)
        for ref in part_refs[1:]:
            proj = proj + ref[...].astype(jnp.float32)
        middle = (tokens_ref[...].astype(jnp.float32) + proj).astype(jnp.bfloat16)
        wide = middle.astype(jnp.float32)
        scratch[...] = wide
        column = aligned(lax.axis_index("tp"), col_width)
        middle_ref[...] = scratch[:, pl.ds(column, col_width)]
        mean_square = jnp.mean(wide * wide, axis=-1, keepdims=True)
        normed = (wide * lax.rsqrt(mean_square + epsilon) * gain_ref[...]).astype(jnp.bfloat16)
        outbox = jnp.dot(
            picks_ref[:, :rows], normed, preferred_element_type=jnp.float32
        ).astype(jnp.bfloat16)
        kept_ref[:, :width] = outbox[:slots]
        away_ref[:, :width] = outbox[slots:]
        kept_ref[:, width:] = notes_ref[:slots]
        away_ref[:, width:] = notes_ref[slots:]

    shape = (slots, width + LANES)
    return pl.pallas_call(
        kernel,
        out_shape=[
            jax.ShapeDtypeStruct((rows, col_width), jnp.float32),
            jax.ShapeDtypeStruct(shape, jnp.bfloat16),
            jax.ShapeDtypeStruct(shape, jnp.bfloat16),
        ],
        in_specs=in_vmem(terms + 4),
        out_specs=in_vmem(3),
        scratch_shapes=[pltpu.VMEM((rows, width), jnp.float32)],
        compiler_params=pltpu.CompilerParams(vmem_limit_bytes=8 << 20),
    )(picks, notes, tokens, *attn_parts, mix_gain.reshape(1, -1))


def experts_apply(parts, gate_up, down, side_in, side_back, branch_gate, capacity):
    count, tp_size = lax.axis_size("ep"), lax.axis_size("tp")
    width = parts[0].shape[1] - LANES
    col_width = width // tp_size
    chunks = col_width // LANES

    def kernel(*refs):
        part_refs = refs[: len(parts)]
        gate_up_ref, down_ref, side_in_ref, side_back_ref, branch_ref, out_ref = refs[len(parts) :]
        whole = jnp.concatenate([ref[...] for ref in part_refs], axis=0)
        lines = whole[:, :width]
        notes = whole[:, width:].astype(jnp.float32)
        share = notes[:, 0:1] + notes[:, 1:2]
        logit = jnp.sum(lines.astype(jnp.float32) * branch_ref[...], axis=1, keepdims=True)
        switch = notes[:, 2:3] * jax.nn.sigmoid(logit)

        def hidden_of(gate_pre, up_pre):
            return (jax.nn.silu(gate_pre) * up_pre).astype(jnp.bfloat16)

        both = jnp.dot(lines, gate_up_ref[...], preferred_element_type=jnp.float32)
        units = both.shape[1] // 2
        hidden = hidden_of(both[:, :units], both[:, units:])
        side_hidden = hidden_of(
            jnp.dot(lines, side_in_ref[:width, :], preferred_element_type=jnp.float32),
            jnp.dot(lines, side_in_ref[width:, :], preferred_element_type=jnp.float32),
        )
        high, low = place()
        for t in range(tp_size):
            columns = slice(t * col_width, (t + 1) * col_width)
            result = share * jnp.dot(
                hidden, down_ref[:, columns], preferred_element_type=jnp.float32
            ) + switch * jnp.dot(
                side_hidden, side_back_ref[:, columns], preferred_element_type=jnp.float32
            )
            for step in range(count // 2):
                for part in range(2):
                    source = 2 * (high ^ step) + (low ^ part)
                    start = (2 * step + part) * capacity
                    block = jnp.concatenate(
                        [
                            result[start : start + capacity, c * LANES : (c + 1) * LANES]
                            for c in range(chunks)
                        ],
                        axis=0,
                    )
                    out_ref[source * tp_size + t] = block.astype(jnp.bfloat16)

    shape = (count * tp_size, chunks * capacity, LANES)
    return call(
        kernel,
        [(shape, jnp.bfloat16)],
        *parts,
        gate_up,
        down,
        side_in,
        side_back,
        branch_gate.reshape(1, -1),
        limit=12 << 20,
    )[0]


def home_picks(ids, rows, capacity, chunks):
    count, tp_size = lax.axis_size("ep"), lax.axis_size("tp")
    per_block = chunks * capacity
    total = count * tp_size * per_block

    def kernel(ids_ref, out_ref):
        row = lax.broadcasted_iota(jnp.int32, (chunks * rows, total), 0)
        column = lax.broadcasted_iota(jnp.int32, (chunks * rows, total), 1)
        expert_of = lax.div(column, jnp.int32(tp_size * per_block))
        within = lax.rem(column, jnp.int32(per_block))
        same = lax.div(within, jnp.int32(capacity)) == lax.div(row, jnp.int32(rows))
        key = expert_of * capacity + lax.rem(within, jnp.int32(capacity))
        token = lax.rem(row, jnp.int32(rows))
        picks = jnp.zeros((chunks * rows, total), jnp.float32)
        for b, _, expert, slot in slots_of(ids_ref):
            hit = (key == expert * capacity + slot) & (token == b)
            picks = jnp.where(hit, 1.0, picks)
        out_ref[...] = jnp.where(same, picks, 0.0).astype(jnp.bfloat16)

    shape = (chunks * rows, total)
    return call(kernel, [(shape, jnp.bfloat16)], ids, scalars=1)[0]


def finish(picks, returned, middle):
    rows, col_width = middle.shape
    chunks = col_width // LANES

    def kernel(picks_ref, returned_ref, middle_ref, out_ref):
        lines = returned_ref[...].reshape(-1, LANES)
        sums = jnp.dot(picks_ref[...], lines, preferred_element_type=jnp.float32)
        for c in range(chunks):
            columns = slice(c * LANES, (c + 1) * LANES)
            total = middle_ref[:, columns] + sums[c * rows : (c + 1) * rows]
            out_ref[:, columns] = total.astype(jnp.bfloat16)

    return call(kernel, [((rows, col_width), jnp.bfloat16)], picks, returned, middle)[0]


def fast_layer(
    tokens,
    attn_gain,
    query_weight,
    key_weight,
    value_weight,
    query_gain,
    stick_bias,
    key_cache,
    value_cache,
    lengths,
    out_weight,
    mix_gain,
    route_ids,
    route_weights,
    expert_gate,
    expert_up,
    expert_down,
    side_gate,
    side_up,
    side_down,
    branch_gate,
):
    seq_count, model_width = tokens.shape
    head_cols = query_weight.shape[1]
    heads_local = key_cache.shape[1]
    cache_slots = key_cache.shape[2]
    experts, tp_size = lax.axis_size("ep"), lax.axis_size("tp")
    half = experts // 2
    top_count = route_ids.shape[1]
    capacity = max(2, 2 * top_count * seq_count // experts)

    came = pair_move(tokens)
    scales = row_scales(tokens)
    parts = knit(tokens, came)
    parts = [parts[0]] + [far_move(parts[step], step) for step in range(1, half)]
    turned_keys, weights = stage_keys(key_cache, query_weight, key_weight, value_weight)
    away, kept = project(parts, attn_gain, weights, 3)
    came = pair_move(away)
    both = kept + came.astype(jnp.float32)
    projected = both[:seq_count]
    for step in range(1, half):
        leaving = both[step * seq_count : (step + 1) * seq_count].astype(jnp.bfloat16)
        moved = far_move(leaving, step)
        projected = projected + moved.astype(jnp.float32)
    projected = (projected * scales[:, :1]).astype(jnp.bfloat16)
    query_rows = projected[:, :head_cols]
    fresh_keys = projected[:, head_cols : 2 * head_cols].astype(jnp.float32)
    new_values = projected[:, 2 * head_cols :]
    new_keys = rms_scale(fresh_keys.reshape(seq_count, heads_local, DH), 1.0)
    new_keys = new_keys.astype(jnp.bfloat16).reshape(seq_count, head_cols)
    query_heads = rms_scale(
        query_rows.astype(jnp.float32).reshape(seq_count, heads_local, DH), query_gain
    ).astype(jnp.bfloat16)
    (value_cache,) = stage([value_cache])

    scores = jnp.einsum(
        "shd,shdl->shl", query_heads, turned_keys, preferred_element_type=jnp.float32
    )
    scores = scores * DH ** (-0.5) + stick_bias[None, :, None]
    positions = jnp.arange(cache_slots, dtype=jnp.int32)
    visible = positions[None, None, :] < lengths[:, None, None]
    log_rest = jnp.where(visible, jax.nn.log_sigmoid(-scores), 0.0)
    later = (positions[:, None] > positions[None, :]).astype(jnp.float32)
    log_between = jnp.dot(
        log_rest.reshape(-1, cache_slots), later, precision=lax.Precision.HIGHEST
    ).reshape(scores.shape)
    stick = jnp.where(visible, jnp.exp(jax.nn.log_sigmoid(scores) + log_between), 0.0).astype(
        jnp.bfloat16
    )
    attended = jnp.einsum("shl,shld->shd", stick, value_cache, preferred_element_type=jnp.float32)
    attended = attended.astype(jnp.bfloat16).reshape(seq_count, head_cols)
    attn_part = jnp.dot(attended, out_weight, preferred_element_type=jnp.float32)
    attn_part = attn_part.astype(jnp.bfloat16)
    attn_parts = [attn_part] + [tp_move(attn_part, turn) for turn in range(1, tp_size)]
    ids = route_ids.T
    plan_outs, plan_work = plan_sends(capacity)
    side_in, side_back, picks, notes = stage(
        [side_gate, side_up],
        [side_down],
        scalars=(ids, route_weights.T),
        outs=plan_outs,
        work=plan_work,
    )
    middle, kept, away = dispatch(picks, notes, tokens, attn_parts, mix_gain)
    came = pair_move(away)
    kept = kept.reshape(half, capacity, -1)
    came = came.reshape(half, capacity, -1)
    parts = [jnp.concatenate([kept[step], came[step]], axis=0) for step in range(half)]
    parts = [parts[0]] + [far_move(parts[step], step) for step in range(1, half)]
    (gate_up,) = stage_beside((expert_gate[0], expert_up[0]))
    blocks = experts_apply(
        parts, gate_up, expert_down[0], side_in, side_back, branch_gate, capacity
    )
    returned = lax.all_to_all(
        blocks, ("ep", "tp"), split_axis=0, concat_axis=0, tiled=True
    )
    picks = home_picks(ids, seq_count, capacity, model_width // tp_size // LANES)
    mixed = finish(picks, returned, middle)
    return (mixed, new_keys, new_values)


def two_power(count):
    return count & (count - 1) == 0


def body(*arrays):
    tokens = arrays[0]
    experts, tp_size = lax.axis_size("ep"), lax.axis_size("tp")
    widths = (tokens.shape[1] // experts, tokens.shape[1] // tp_size, arrays[14].shape[2])
    fits = experts > 1 and two_power(experts) and two_power(tp_size)
    fits = fits and all(width % LANES == 0 for width in widths)
    fits = fits and tokens.shape[0] == 8
    return (fast_layer if fits else plain_layer)(*arrays)


def solution(mesh):
    in_specs = (
        P("ep", None),
        P(),
        P("ep", "tp"),
        P("ep", "tp"),
        P("ep", "tp"),
        P(),
        P("tp"),
        P("ep", "tp", None, None),
        P("ep", "tp", None, None),
        P("ep"),
        P("tp", None),
        P(),
        P("ep", None),
        P("ep", None),
        P("ep", None, "tp"),
        P("ep", None, "tp"),
        P("ep", "tp", None),
        P(None, "tp"),
        P(None, "tp"),
        P("tp", None),
        P(),
    )
    out_specs = (P("ep", "tp"), P("ep", "tp"), P("ep", "tp"))
    return jax.shard_map(body, mesh=mesh, in_specs=in_specs, out_specs=out_specs, check_vma=False)
```

```python
import jax
import jax.numpy as jnp
from jax import lax
from jax.experimental import pallas as pl
from jax.experimental.pallas import tpu as pltpu
from jax.sharding import PartitionSpec as P


DH = 128
COPY_BYTES = 1 << 20
LANES = 128


epsilon = 1e-06


def rms_scale(values, scale_gain):
    mean_square = jnp.mean(values * values, axis=-1, keepdims=True)
    return values * lax.rsqrt(mean_square + epsilon) * scale_gain


def summed_blocks(partial, axis_name):
    count = lax.axis_size(axis_name)
    rows = partial.shape[0] // count
    blocks = lax.all_to_all(
        partial.astype(jnp.bfloat16), axis_name, split_axis=0, concat_axis=0, tiled=True
    )
    return jnp.sum(blocks.reshape(count, rows, -1).astype(jnp.float32), axis=0)


def plain_layer(
    tokens,
    attn_gain,
    query_weight,
    key_weight,
    value_weight,
    query_gain,
    stick_bias,
    key_cache,
    value_cache,
    lengths,
    out_weight,
    mix_gain,
    route_ids,
    route_weights,
    expert_gate,
    expert_up,
    expert_down,
    side_gate,
    side_up,
    side_down,
    branch_gate,
):
    seq_count, model_width = tokens.shape
    head_cols = query_weight.shape[1]
    heads_local = key_cache.shape[1]
    cache_slots = key_cache.shape[2]
    experts = lax.axis_size("ep")
    tp_size = lax.axis_size("tp")
    stream = tokens.astype(jnp.float32)
    normed = rms_scale(stream, attn_gain).astype(jnp.bfloat16)
    columns = lax.all_to_all(normed, "ep", split_axis=1, concat_axis=0, tiled=True)
    query_rows = summed_blocks(
        jnp.dot(columns, query_weight, preferred_element_type=jnp.float32), "ep"
    ).astype(jnp.bfloat16)
    query_heads = rms_scale(
        query_rows.astype(jnp.float32).reshape(seq_count, heads_local, DH), query_gain
    ).astype(jnp.bfloat16)
    fresh = jnp.concatenate(
        [
            jnp.dot(columns, key_weight, preferred_element_type=jnp.float32),
            jnp.dot(columns, value_weight, preferred_element_type=jnp.float32),
        ],
        axis=1,
    )
    fresh = summed_blocks(fresh, "ep").astype(jnp.bfloat16)
    new_values = fresh[:, head_cols:]
    new_keys = rms_scale(
        fresh[:, :head_cols].astype(jnp.float32).reshape(seq_count, heads_local, DH), 1.0
    )
    new_keys = new_keys.astype(jnp.bfloat16).reshape(seq_count, head_cols)

    scores = jnp.einsum("shd,shld->shl", query_heads, key_cache, preferred_element_type=jnp.float32)
    scores = scores * DH ** (-0.5) + stick_bias[None, :, None]
    positions = jnp.arange(cache_slots, dtype=jnp.int32)
    visible = positions[None, None, :] < lengths[:, None, None]
    log_rest = jnp.where(visible, jax.nn.log_sigmoid(-scores), 0.0)
    later = (positions[:, None] > positions[None, :]).astype(jnp.float32)
    log_between = jnp.dot(
        log_rest.reshape(-1, cache_slots), later, precision=lax.Precision.HIGHEST
    ).reshape(scores.shape)
    stick = jnp.where(visible, jnp.exp(jax.nn.log_sigmoid(scores) + log_between), 0.0).astype(
        jnp.bfloat16
    )
    attended = jnp.einsum("shl,shld->shd", stick, value_cache, preferred_element_type=jnp.float32)
    attended = attended.astype(jnp.bfloat16).reshape(seq_count, head_cols)
    attn_part = jnp.dot(attended, out_weight, preferred_element_type=jnp.float32)
    attn_parts = lax.all_gather(attn_part.astype(jnp.bfloat16), "tp", axis=0, tiled=False)
    attn_proj = jnp.sum(attn_parts.astype(jnp.float32), axis=0)
    middle = (stream + attn_proj).astype(jnp.bfloat16)
    normed_mix = rms_scale(middle.astype(jnp.float32), mix_gain).astype(jnp.bfloat16)

    top_count = route_ids.shape[1]
    capacity = max(2, 2 * top_count * seq_count // experts)
    slots = experts * capacity
    flat_ids = route_ids.reshape(-1)
    onehot = (flat_ids[:, None] == jnp.arange(experts, dtype=jnp.int32)[None, :]).astype(jnp.int32)
    order = jnp.arange(flat_ids.shape[0], dtype=jnp.int32)
    earlier = (order[:, None] > order[None, :]) & (flat_ids[:, None] == flat_ids[None, :])
    slot_index = jnp.sum(earlier.astype(jnp.int32), axis=1)
    target = flat_ids * capacity + slot_index
    route_map = (target[:, None] == jnp.arange(slots, dtype=jnp.int32)[None, :]).astype(
        jnp.bfloat16
    )
    dispatch = jnp.sum(route_map.reshape(seq_count, top_count, slots), axis=1).T
    outbox = jnp.dot(dispatch, normed_mix, preferred_element_type=jnp.float32).astype(jnp.bfloat16)
    slot_rows = lax.all_to_all(outbox, "ep", split_axis=0, concat_axis=0, tiled=True)

    side_gate_pre = jnp.dot(normed_mix, side_gate, preferred_element_type=jnp.float32)
    side_up_pre = jnp.dot(normed_mix, side_up, preferred_element_type=jnp.float32)
    side_hidden = (jax.nn.silu(side_gate_pre) * side_up_pre).astype(jnp.bfloat16)
    side_term = jnp.dot(side_hidden, side_down, preferred_element_type=jnp.float32)
    switch = jax.nn.sigmoid(
        jnp.sum(normed_mix.astype(jnp.float32) * branch_gate, axis=1, keepdims=True)
    )
    col_width = model_width // tp_size
    col_offset = lax.axis_index("tp") * col_width
    side_blocks = lax.all_to_all(
        side_term.astype(jnp.bfloat16).reshape(seq_count, tp_size, col_width).transpose(1, 0, 2),
        "tp",
        split_axis=0,
        concat_axis=0,
        tiled=True,
    )
    side_part = jnp.sum(side_blocks.astype(jnp.float32), axis=0)

    gate_pre = jnp.dot(slot_rows, expert_gate[0], preferred_element_type=jnp.float32)
    up_pre = jnp.dot(slot_rows, expert_up[0], preferred_element_type=jnp.float32)
    hidden = (jax.nn.silu(gate_pre) * up_pre).astype(jnp.bfloat16)
    expert_term = jnp.dot(hidden, expert_down[0], preferred_element_type=jnp.float32)
    expert_term = expert_term.astype(jnp.bfloat16).reshape(experts, capacity, tp_size, col_width)
    returned = lax.all_to_all(
        expert_term.transpose(0, 2, 1, 3).reshape(experts * tp_size, capacity, col_width),
        ("ep", "tp"),
        split_axis=0,
        concat_axis=0,
        tiled=True,
    )
    expert_out = jnp.sum(
        returned.reshape(experts, tp_size, capacity, col_width).astype(jnp.float32), axis=1
    ).astype(jnp.bfloat16)
    picked = jnp.dot(
        route_map, expert_out.reshape(slots, col_width), preferred_element_type=jnp.float32
    )
    routed = jnp.sum(
        route_weights[:, :, None] * picked.reshape(seq_count, top_count, col_width), axis=1
    )
    middle_cols = lax.dynamic_slice_in_dim(middle, col_offset, col_width, 1).astype(jnp.float32)
    mixed = (middle_cols + routed + switch * side_part).astype(jnp.bfloat16)
    return (mixed, new_keys, new_values)


def in_vmem(count):
    return [pl.BlockSpec(memory_space=pltpu.VMEM)] * count


def call(kernel, outs, *arrays, scalars=0, limit=8 << 20):
    return pl.pallas_call(
        kernel,
        out_shape=[jax.ShapeDtypeStruct(shape, dtype) for shape, dtype in outs],
        in_specs=[pl.BlockSpec(memory_space=pltpu.SMEM)] * scalars
        + in_vmem(len(arrays) - scalars),
        out_specs=in_vmem(len(outs)),
        compiler_params=pltpu.CompilerParams(vmem_limit_bytes=limit),
    )(*arrays)


def stage(*groups, scalars=(), outs=(), work=None):
    plan, shapes = [], []
    for target, group in enumerate(groups):
        offset = 0
        for array in group:
            size = array.size * array.dtype.itemsize
            count = max(1, size // COPY_BYTES)
            while array.shape[0] % count:
                count -= 1
            plan.append((target, offset, array.shape[0] // count, count))
            offset += array.shape[0]
        shapes.append(pltpu.VMEM((offset,) + group[0].shape[1:], group[0].dtype))
    arrays = [array for group in groups for array in group]
    total = sum(count for *_, count in plan)

    def kernel(*refs):
        scalar_refs, refs = refs[: len(scalars)], refs[len(scalars) :]
        sources, sems = refs[: len(arrays)], refs[-1]
        targets = refs[len(arrays) : len(arrays) + len(groups)]
        copies = []
        for source, (target, offset, rows, count) in zip(sources, plan):
            for i in range(count):
                copies.append(
                    pltpu.make_async_copy(
                        source.at[pl.ds(i * rows, rows)],
                        targets[target].at[pl.ds(offset + i * rows, rows)],
                        sems.at[len(copies)],
                    )
                )
        for copy in copies:
            copy.start()
        if work is not None:
            work(*scalar_refs, *refs[len(arrays) + len(groups) : -1])
        for copy in copies:
            copy.wait()

    return pl.pallas_call(
        kernel,
        out_shape=shapes + [jax.ShapeDtypeStruct(shape, dtype) for shape, dtype in outs],
        in_specs=[pl.BlockSpec(memory_space=pltpu.SMEM)] * len(scalars)
        + [pl.BlockSpec(memory_space=pltpu.HBM) for _ in arrays],
        out_specs=in_vmem(len(groups) + len(outs)),
        scratch_shapes=[pltpu.SemaphoreType.DMA((total,))],
        compiler_params=pltpu.CompilerParams(vmem_limit_bytes=1 << 20),
    )(*scalars, *[pltpu.with_memory_space_constraint(array, pltpu.HBM) for array in arrays])


def stage_keys(keys, *arrays):
    seqs, heads, slots, size = keys.shape
    rows = [array.shape[0] for array in arrays]

    def kernel(keys_ref, *refs):
        array_refs = refs[: len(arrays)]
        turned_ref, stacked_ref, scratch, key_sems, array_sems = refs[len(arrays) :]
        key_copies = [
            pltpu.make_async_copy(keys_ref.at[s], scratch.at[s], key_sems.at[s])
            for s in range(seqs)
        ]
        array_copies = [
            pltpu.make_async_copy(
                ref, stacked_ref.at[pl.ds(sum(rows[:i]), rows[i])], array_sems.at[i]
            )
            for i, ref in enumerate(array_refs)
        ]
        for copy in key_copies + array_copies:
            copy.start()
        for s in range(seqs):
            key_copies[s].wait()
            for h in range(heads):
                turned_ref[s, h] = scratch[s, h].T
        for copy in array_copies:
            copy.wait()

    return pl.pallas_call(
        kernel,
        out_shape=[
            pltpu.VMEM((seqs, heads, size, slots), keys.dtype),
            pltpu.VMEM((sum(rows),) + arrays[0].shape[1:], arrays[0].dtype),
        ],
        in_specs=[pl.BlockSpec(memory_space=pltpu.HBM)] * (1 + len(arrays)),
        out_specs=in_vmem(2),
        scratch_shapes=[
            pltpu.VMEM(keys.shape, keys.dtype),
            pltpu.SemaphoreType.DMA((seqs,)),
            pltpu.SemaphoreType.DMA((len(arrays),)),
        ],
        compiler_params=pltpu.CompilerParams(vmem_limit_bytes=16 << 20),
    )(*[pltpu.with_memory_space_constraint(array, pltpu.HBM) for array in (keys, *arrays)])


def stage_beside(*pairs):
    def kernel(*refs):
        sources, targets, sems = refs[: 2 * len(pairs)], refs[2 * len(pairs) : -1], refs[-1]
        copies = []
        for n, target in enumerate(targets):
            rows, width = sources[2 * n].shape
            pieces = 4 if rows % 64 == 0 else 1
            for k in range(2):
                for i in range(pieces):
                    part = pl.ds(i * (rows // pieces), rows // pieces)
                    copies.append(
                        pltpu.make_async_copy(
                            sources[2 * n + k].at[part],
                            target.at[part, pl.ds(k * width, width)],
                            sems.at[len(copies)],
                        )
                    )
        for copy in copies:
            copy.start()
        for copy in copies:
            copy.wait()

    arrays = [array for pair in pairs for array in pair]
    return pl.pallas_call(
        kernel,
        out_shape=[
            pltpu.VMEM((pair[0].shape[0], 2 * pair[0].shape[1]), pair[0].dtype) for pair in pairs
        ],
        in_specs=[pl.BlockSpec(memory_space=pltpu.HBM)] * len(arrays),
        out_specs=in_vmem(len(pairs)),
        scratch_shapes=[pltpu.SemaphoreType.DMA((8 * len(pairs),))],
        compiler_params=pltpu.CompilerParams(vmem_limit_bytes=1 << 20),
    )(*[pltpu.with_memory_space_constraint(array, pltpu.HBM) for array in arrays])


def place():
    index = lax.axis_index("ep")
    return lax.div(index, jnp.int32(2)), lax.rem(index, jnp.int32(2))


def pair_move(values):
    count = lax.axis_size("ep")
    return lax.ppermute(values, "ep", [(i, i ^ 1) for i in range(count)])


def far_move(values, step):
    count = lax.axis_size("ep")
    return lax.ppermute(values, "ep", [(i, i ^ (2 * step)) for i in range(count)])


def tp_move(values, turn):
    count = lax.axis_size("tp")
    return lax.ppermute(values, "tp", [(i, i ^ turn) for i in range(count)])


def aligned(index, size):
    return pl.multiple_of(index * size, size)


def row_scales(tokens):
    def kernel(tokens_ref, scale_ref):
        stream = tokens_ref[...].astype(jnp.float32)
        mean_square = jnp.mean(stream * stream, axis=-1, keepdims=True)
        scale_ref[...] = jnp.broadcast_to(lax.rsqrt(mean_square + epsilon), scale_ref.shape)

    return call(kernel, [((tokens.shape[0], LANES), jnp.float32)], tokens)[0]


def knit(tokens, came):
    rows, width = tokens.shape
    count = lax.axis_size("ep")
    features = width // count
    half = count // 2

    def kernel(tokens_ref, came_ref, *outs):
        high, low = place()
        for step, out_ref in enumerate(outs):
            part = pl.ds(aligned(2 * (high ^ step) + low, features), features)
            out_ref[...] = jnp.concatenate([tokens_ref[:, part], came_ref[:, part]], axis=0)

    return call(kernel, [((2 * rows, features), tokens.dtype)] * half, tokens, came)


def project(parts, gain, weights, parts_out):
    features = parts[0].shape[1]
    rows = parts[0].shape[0] // 2
    half = len(parts)
    wide = weights.shape[1]

    def kernel(*refs):
        part_refs, (gain_ref, weight_ref, away_ref, kept_ref) = refs[:half], refs[half:]
        gain_part = gain_ref[:, pl.ds(aligned(lax.axis_index("ep"), features), features)]
        values = [ref[...].astype(jnp.float32) for ref in part_refs]
        ordered = [value[rows:] for value in values] + [value[:rows] for value in values]
        lines = (jnp.concatenate(ordered, axis=0) * gain_part).astype(jnp.bfloat16)
        for i in range(parts_out):
            weight = weight_ref[i * features : (i + 1) * features, :]
            part = jnp.dot(lines, weight, preferred_element_type=jnp.float32)
            away_ref[:, i * wide : (i + 1) * wide] = part[: half * rows].astype(jnp.bfloat16)
            kept_ref[:, i * wide : (i + 1) * wide] = part[half * rows :]

    shape = (half * rows, parts_out * wide)
    return call(
        kernel,
        [(shape, jnp.bfloat16), (shape, jnp.float32)],
        *parts,
        gain.reshape(1, -1),
        weights,
        limit=16 << 20,
    )


def slots_of(ids_ref):
    chosen = []
    for b in range(ids_ref.shape[1]):
        for k in range(ids_ref.shape[0]):
            expert = ids_ref[k, b]
            slot = jnp.int32(0)
            for _, _, other, _ in chosen:
                slot = slot + (other == expert).astype(jnp.int32)
            chosen.append((b, k, expert, slot))
    return chosen


def plan_sends(capacity):
    half = lax.axis_size("ep") // 2
    slots = half * capacity

    def kernel(ids_ref, weights_ref, picks_ref, notes_ref):
        high, low = place()
        line = lax.broadcasted_iota(jnp.int32, (2 * slots, LANES), 0)
        lane = lax.broadcasted_iota(jnp.int32, (2 * slots, LANES), 1)
        picks = jnp.zeros((2 * slots, LANES), jnp.float32)
        share = jnp.zeros((2 * slots, LANES), jnp.float32)
        first = jnp.zeros((2 * slots, LANES), jnp.float32)
        for b, k, expert, slot in slots_of(ids_ref):
            block = lax.div(expert, jnp.int32(2)) ^ high
            side = lax.rem(expert, jnp.int32(2)) ^ low
            here = line == side * slots + block * capacity + slot
            picks = jnp.where(here & (lane == b), 1.0, picks)
            share = jnp.where(here, weights_ref[k, b], share)
            if k == 0:
                first = jnp.where(here, 1.0, first)
        upper = share.astype(jnp.bfloat16).astype(jnp.float32)
        notes = jnp.where(lane == 0, upper, jnp.where(lane == 1, share - upper, first))
        picks_ref[...] = picks.astype(jnp.bfloat16)
        notes_ref[...] = notes.astype(jnp.bfloat16)

    shape = (2 * slots, LANES)
    return [(shape, jnp.bfloat16), (shape, jnp.bfloat16)], kernel


def dispatch(picks, notes, tokens, attn_parts, mix_gain):
    rows, width = tokens.shape
    col_width = width // lax.axis_size("tp")
    slots = picks.shape[0] // 2
    terms = len(attn_parts)

    def kernel(picks_ref, notes_ref, tokens_ref, *refs):
        part_refs, gain_ref = refs[:terms], refs[terms]
        middle_ref, kept_ref, away_ref, scratch = refs[terms + 1 :]
        proj = part_refs[0][...].astype(jnp.float32)
        for ref in part_refs[1:]:
            proj = proj + ref[...].astype(jnp.float32)
        middle = (tokens_ref[...].astype(jnp.float32) + proj).astype(jnp.bfloat16)
        wide = middle.astype(jnp.float32)
        scratch[...] = wide
        column = aligned(lax.axis_index("tp"), col_width)
        middle_ref[...] = scratch[:, pl.ds(column, col_width)]
        mean_square = jnp.mean(wide * wide, axis=-1, keepdims=True)
        normed = (wide * lax.rsqrt(mean_square + epsilon) * gain_ref[...]).astype(jnp.bfloat16)
        outbox = jnp.dot(
            picks_ref[:, :rows], normed, preferred_element_type=jnp.float32
        ).astype(jnp.bfloat16)
        kept_ref[:, :width] = outbox[:slots]
        away_ref[:, :width] = outbox[slots:]
        kept_ref[:, width:] = notes_ref[:slots]
        away_ref[:, width:] = notes_ref[slots:]

    shape = (slots, width + LANES)
    return pl.pallas_call(
        kernel,
        out_shape=[
            jax.ShapeDtypeStruct((rows, col_width), jnp.float32),
            jax.ShapeDtypeStruct(shape, jnp.bfloat16),
            jax.ShapeDtypeStruct(shape, jnp.bfloat16),
        ],
        in_specs=in_vmem(terms + 4),
        out_specs=in_vmem(3),
        scratch_shapes=[pltpu.VMEM((rows, width), jnp.float32)],
        compiler_params=pltpu.CompilerParams(vmem_limit_bytes=8 << 20),
    )(picks, notes, tokens, *attn_parts, mix_gain.reshape(1, -1))


def experts_apply(parts, gate_up, down, side_in, side_back, branch_gate, capacity):
    count, tp_size = lax.axis_size("ep"), lax.axis_size("tp")
    width = parts[0].shape[1] - LANES
    col_width = width // tp_size
    chunks = col_width // LANES

    def kernel(*refs):
        part_refs = refs[: len(parts)]
        gate_up_ref, down_ref, side_in_ref, side_back_ref, branch_ref, out_ref = refs[len(parts) :]
        whole = jnp.concatenate([ref[...] for ref in part_refs], axis=0)
        lines = whole[:, :width]
        notes = whole[:, width:].astype(jnp.float32)
        share = notes[:, 0:1] + notes[:, 1:2]
        logit = jnp.sum(lines.astype(jnp.float32) * branch_ref[...], axis=1, keepdims=True)
        switch = notes[:, 2:3] * jax.nn.sigmoid(logit)

        def hidden_of(gate_pre, up_pre):
            return (jax.nn.silu(gate_pre) * up_pre).astype(jnp.bfloat16)

        both = jnp.dot(lines, gate_up_ref[...], preferred_element_type=jnp.float32)
        units = both.shape[1] // 2
        hidden = hidden_of(both[:, :units], both[:, units:])
        side_hidden = hidden_of(
            jnp.dot(lines, side_in_ref[:width, :], preferred_element_type=jnp.float32),
            jnp.dot(lines, side_in_ref[width:, :], preferred_element_type=jnp.float32),
        )
        high, low = place()
        for t in range(tp_size):
            columns = slice(t * col_width, (t + 1) * col_width)
            result = share * jnp.dot(
                hidden, down_ref[:, columns], preferred_element_type=jnp.float32
            ) + switch * jnp.dot(
                side_hidden, side_back_ref[:, columns], preferred_element_type=jnp.float32
            )
            for step in range(count // 2):
                for part in range(2):
                    source = 2 * (high ^ step) + (low ^ part)
                    start = (2 * step + part) * capacity
                    block = jnp.concatenate(
                        [
                            result[start : start + capacity, c * LANES : (c + 1) * LANES]
                            for c in range(chunks)
                        ],
                        axis=0,
                    )
                    out_ref[source * tp_size + t] = block.astype(jnp.bfloat16)

    shape = (count * tp_size, chunks * capacity, LANES)
    return call(
        kernel,
        [(shape, jnp.bfloat16)],
        *parts,
        gate_up,
        down,
        side_in,
        side_back,
        branch_gate.reshape(1, -1),
        limit=12 << 20,
    )[0]


def home_picks(ids, rows, capacity, chunks):
    count, tp_size = lax.axis_size("ep"), lax.axis_size("tp")
    per_block = chunks * capacity
    total = count * tp_size * per_block

    def kernel(ids_ref, out_ref):
        row = lax.broadcasted_iota(jnp.int32, (chunks * rows, total), 0)
        column = lax.broadcasted_iota(jnp.int32, (chunks * rows, total), 1)
        expert_of = lax.div(column, jnp.int32(tp_size * per_block))
        within = lax.rem(column, jnp.int32(per_block))
        same = lax.div(within, jnp.int32(capacity)) == lax.div(row, jnp.int32(rows))
        key = expert_of * capacity + lax.rem(within, jnp.int32(capacity))
        token = lax.rem(row, jnp.int32(rows))
        picks = jnp.zeros((chunks * rows, total), jnp.float32)
        for b, _, expert, slot in slots_of(ids_ref):
            hit = (key == expert * capacity + slot) & (token == b)
            picks = jnp.where(hit, 1.0, picks)
        out_ref[...] = jnp.where(same, picks, 0.0).astype(jnp.bfloat16)

    shape = (chunks * rows, total)
    return call(kernel, [(shape, jnp.bfloat16)], ids, scalars=1)[0]


def finish(picks, returned, middle):
    rows, col_width = middle.shape
    chunks = col_width // LANES

    def kernel(picks_ref, returned_ref, middle_ref, out_ref):
        lines = returned_ref[...].reshape(-1, LANES)
        sums = jnp.dot(picks_ref[...], lines, preferred_element_type=jnp.float32)
        for c in range(chunks):
            columns = slice(c * LANES, (c + 1) * LANES)
            total = middle_ref[:, columns] + sums[c * rows : (c + 1) * rows]
            out_ref[:, columns] = total.astype(jnp.bfloat16)

    return call(kernel, [((rows, col_width), jnp.bfloat16)], picks, returned, middle)[0]


def fast_layer(
    tokens,
    attn_gain,
    query_weight,
    key_weight,
    value_weight,
    query_gain,
    stick_bias,
    key_cache,
    value_cache,
    lengths,
    out_weight,
    mix_gain,
    route_ids,
    route_weights,
    expert_gate,
    expert_up,
    expert_down,
    side_gate,
    side_up,
    side_down,
    branch_gate,
):
    seq_count, model_width = tokens.shape
    head_cols = query_weight.shape[1]
    heads_local = key_cache.shape[1]
    cache_slots = key_cache.shape[2]
    experts, tp_size = lax.axis_size("ep"), lax.axis_size("tp")
    half = experts // 2
    top_count = route_ids.shape[1]
    capacity = max(2, 2 * top_count * seq_count // experts)

    came = pair_move(tokens)
    scales = row_scales(tokens)
    parts = knit(tokens, came)
    moved_parts = [parts[0]]
    for step in range(1, half):
        moved_parts.append(far_move(parts[step], step))
    parts = moved_parts
    turned_keys, weights = stage_keys(key_cache, query_weight, key_weight, value_weight)
    away, kept = project(parts, attn_gain, weights, 3)
    came = pair_move(away)
    both = kept + came.astype(jnp.float32)
    projected = both[:seq_count]
    for step in range(1, half):
        leaving = both[step * seq_count : (step + 1) * seq_count].astype(jnp.bfloat16)
        moved = far_move(leaving, step)
        projected = projected + moved.astype(jnp.float32)
    projected = (projected * scales[:, :1]).astype(jnp.bfloat16)
    query_rows = projected[:, :head_cols]
    fresh_keys = projected[:, head_cols : 2 * head_cols].astype(jnp.float32)
    new_values = projected[:, 2 * head_cols :]
    new_keys = rms_scale(fresh_keys.reshape(seq_count, heads_local, DH), 1.0)
    new_keys = new_keys.astype(jnp.bfloat16).reshape(seq_count, head_cols)
    query_heads = rms_scale(
        query_rows.astype(jnp.float32).reshape(seq_count, heads_local, DH), query_gain
    ).astype(jnp.bfloat16)
    (value_cache,) = stage([value_cache])

    scores = jnp.einsum(
        "shd,shdl->shl", query_heads, turned_keys, preferred_element_type=jnp.float32
    )
    scores = scores * DH ** (-0.5) + stick_bias[None, :, None]
    positions = jnp.arange(cache_slots, dtype=jnp.int32)
    visible = positions[None, None, :] < lengths[:, None, None]
    log_rest = jnp.where(visible, jax.nn.log_sigmoid(-scores), 0.0)
    later = (positions[:, None] > positions[None, :]).astype(jnp.float32)
    log_between = jnp.dot(
        log_rest.reshape(-1, cache_slots), later, precision=lax.Precision.HIGH
    ).reshape(scores.shape)
    stick = jnp.where(visible, jnp.exp(jax.nn.log_sigmoid(scores) + log_between), 0.0).astype(
        jnp.bfloat16
    )
    attended = jnp.einsum("shl,shld->shd", stick, value_cache, preferred_element_type=jnp.float32)
    attended = attended.astype(jnp.bfloat16).reshape(seq_count, head_cols)
    attn_part = jnp.dot(attended, out_weight, preferred_element_type=jnp.float32)
    attn_part = attn_part.astype(jnp.bfloat16)
    attn_parts = [attn_part]
    for turn in range(1, tp_size):
        attn_parts.append(tp_move(attn_part, turn))
    ids = route_ids.T
    plan_outs, plan_work = plan_sends(capacity)
    side_in, side_back, picks, notes = stage(
        [side_gate, side_up],
        [side_down],
        scalars=(ids, route_weights.T),
        outs=plan_outs,
        work=plan_work,
    )
    middle, kept, away = dispatch(picks, notes, tokens, attn_parts, mix_gain)
    came = pair_move(away)
    kept = kept.reshape(half, capacity, -1)
    came = came.reshape(half, capacity, -1)
    parts = [jnp.concatenate([kept[step], came[step]], axis=0) for step in range(half)]
    moved_parts = [parts[0]]
    for step in range(1, half):
        moved_parts.append(far_move(parts[step], step))
    parts = moved_parts
    (gate_up,) = stage_beside((expert_gate[0], expert_up[0]))
    blocks = experts_apply(
        parts, gate_up, expert_down[0], side_in, side_back, branch_gate, capacity
    )
    returned = lax.all_to_all(
        blocks, ("ep", "tp"), split_axis=0, concat_axis=0, tiled=True
    )
    picks = home_picks(ids, seq_count, capacity, model_width // tp_size // LANES)
    mixed = finish(picks, returned, middle)
    return (mixed, new_keys, new_values)


def two_power(count):
    return count & (count - 1) == 0


def body(*arrays):
    tokens = arrays[0]
    experts, tp_size = lax.axis_size("ep"), lax.axis_size("tp")
    widths = (tokens.shape[1] // experts, tokens.shape[1] // tp_size, arrays[14].shape[2])
    fits = experts > 1 and two_power(experts) and two_power(tp_size)
    fits = fits and all(width % LANES == 0 for width in widths)
    fits = fits and tokens.shape[0] == 8
    return (fast_layer if fits else plain_layer)(*arrays)


def solution(mesh):
    in_specs = (
        P("ep", None),
        P(),
        P("ep", "tp"),
        P("ep", "tp"),
        P("ep", "tp"),
        P(),
        P("tp"),
        P("ep", "tp", None, None),
        P("ep", "tp", None, None),
        P("ep"),
        P("tp", None),
        P(),
        P("ep", None),
        P("ep", None),
        P("ep", None, "tp"),
        P("ep", None, "tp"),
        P("ep", "tp", None),
        P(None, "tp"),
        P(None, "tp"),
        P("tp", None),
        P(),
    )
    out_specs = (P("ep", "tp"), P("ep", "tp"), P("ep", "tp"))
    return jax.shard_map(body, mesh=mesh, in_specs=in_specs, out_specs=out_specs, check_vma=False)
```
